32 devices in a mesh: sp: 8 (over z, x), tp: 4 (over y, core).
Axes of the slice: x: 2, y: 2, z: 4, core: 2. Of those that a mesh axis runs over, the one named last changes fastest.
Arguments:
- tokens: bfloat16 [2048, 2048], P(('sp', 'tp')), may hold values from -40 to 40
- w_query: bfloat16 [2048, 1024], P(None, 'tp'), may hold values from -0.125 to 0.125
- w_key: bfloat16 [2048, 256], P(None, 'tp'), may hold values from -0.125 to 0.125
- w_value: bfloat16 [2048, 256], P(None, 'tp'), may hold values from -0.125 to 0.125
- w_out: bfloat16 [1024, 2048], P('tp'), may hold values from -0.1875 to 0.1875
- cum_gate: float32 [16, 2048], P('tp', 'sp'), may hold values from -295 to 0, as said below
Outputs:
- layer_out: bfloat16 [2048, 2048], P(('sp', 'tp'))
The draws below stay inside these ranges and needn't reach their ends.
Inputs may be any that keep to these rules, and one draw needn't show every extreme that they name: `cum_gate`: each head's row does not rise along the positions.
All inputs are finite; a program needn't handle non-finite values.
Results may differ from the reference program's by a relative error of at most 0.012.
Values may be sent and summed in bfloat16 or wider, within the bound.
A program may use at most 64 MiB of HBM per device.

```python
import math
import jax
import jax.numpy as jnp
from jax import lax

D = 2048
H = 16
KVH = 4
HD = 64
TOK_DEV = 256
STREAM_LENGTH = 2048


def draw_tokens(key, part):
    keys = jax.random.split(key, 3)
    base = jnp.clip(jax.random.normal(keys[0], (STREAM_LENGTH, D), jnp.float32), -6.0, 6.0)
    direction = jnp.clip(jax.random.normal(keys[1], (D,), jnp.float32), -4.0, 4.0)
    level = jax.random.uniform(keys[2], (STREAM_LENGTH // TOK_DEV,), jnp.float32, -1.5, 1.5)
    shifted = jnp.repeat(level, TOK_DEV)
    result = base + shifted[:, None] * direction[None, :]
    return result.astype(jnp.bfloat16)


def draw_cum_gate(key, part):
    keys = jax.random.split(key, 6)
    order = jax.random.permutation(keys[0], H)
    gentle_fading_rate = order < H // 2
    whole_loss = jnp.exp(jax.random.uniform(keys[1], (H,), jnp.float32, math.log(0.3), math.log(1.0)))
    slow_rate = whole_loss / STREAM_LENGTH
    fast_rate = jnp.exp(jax.random.uniform(keys[2], (H,), jnp.float32, math.log(0.01), math.log(1.0 / 30.0)))
    rate = jnp.where(gentle_fading_rate, slow_rate, fast_rate)
    device_multiplier = jnp.exp(jax.random.uniform(keys[3], (STREAM_LENGTH // TOK_DEV,), jnp.float32, math.log(0.5), math.log(2.0)))
    factor_tokens = jnp.repeat(device_multiplier, TOK_DEV)
    rough = jax.random.uniform(keys[4], (H, STREAM_LENGTH), jnp.float32, 0.0, 2.0)
    log_forget_factor = -rate[:, None] * factor_tokens[None, :] * rough
    probe_indices = jax.random.randint(keys[5], (3,), 0, STREAM_LENGTH)
    objective_terms = jax.random.uniform(jax.random.fold_in(key, 9), (3,), jnp.float32, math.log(0.5), math.log(0.8))
    key_head_clusters = jnp.zeros((STREAM_LENGTH,), jnp.float32).at[probe_indices].add(objective_terms)
    log_forget_factor = log_forget_factor + jnp.where(gentle_fading_rate[:, None], key_head_clusters[None, :], 0.0)
    return jnp.cumsum(log_forget_factor, axis=1)


def level_of(rng, dims, cuts, low, largest):
    def one(position, blocks):
        heights = jax.random.uniform(jax.random.fold_in(jax.random.fold_in(rng, 6), position), (blocks,), jnp.float32, low / len(cuts), largest / len(cuts))
        return jnp.repeat(jnp.exp(heights), dims[position] // blocks).reshape((-1,) + (1,) * (len(dims) - position - 1))

    gain = one(*cuts[0])
    for cut in cuts[1:]:
        gain = gain * one(*cut)
    return gain


def scatter_about(key, extent, deviation, bound, cuts=(), kind=jnp.bfloat16):
    values = deviation * jax.random.normal(key, extent, jnp.float32)
    if cuts:
        values = values * level_of(key, extent, cuts, -0.22, 0.18)
    return jnp.clip(values, -bound, bound).astype(kind)


def setup_inputs(seed: int = 0) -> dict:
    key_of = jax.random.split(jax.random.key(seed), 7)
    tokens = draw_tokens(jax.random.fold_in(key_of[6], 71), 0)
    w_query = scatter_about(key_of[1], (D, H * HD), D ** -0.5, 0.125, ((1, 4),))
    w_key = scatter_about(key_of[2], (D, KVH * HD), D ** -0.5, 0.125, ((1, 4),))
    w_value = scatter_about(key_of[3], (D, KVH * HD), D ** -0.5, 0.125, ((1, 4),))
    w_out = scatter_about(key_of[4], (H * HD, D), (H * HD) ** -0.5, 0.1875, ((0, 4),))
    cum_gate = draw_cum_gate(jax.random.fold_in(key_of[6], 71), 0)
    return dict(tokens=tokens, w_query=w_query, w_key=w_key, w_value=w_value, w_out=w_out, cum_gate=cum_gate)


def reference(tokens, w_query, w_key, w_value, w_out, cum_gate):
    length_all = tokens.shape[0]
    queries = jnp.dot(tokens, w_query, preferred_element_type=jnp.float32).astype(jnp.bfloat16)
    key_proj = jnp.dot(tokens, w_key, preferred_element_type=jnp.float32).astype(jnp.bfloat16)
    values = jnp.dot(tokens, w_value, preferred_element_type=jnp.float32).astype(jnp.bfloat16)
    group_size = H // KVH
    block_rows = math.gcd(length_all, 256)
    block_count = length_all // block_rows
    score_factor = float(HD) ** -0.5
    keys_wide = key_proj.astype(jnp.float32).reshape(length_all, KVH, HD)
    values_wide = values.astype(jnp.float32).reshape(length_all, KVH, HD)
    cum_keys = cum_gate.reshape(KVH, group_size, length_all)
    query_blocks = queries.reshape(block_count, block_rows, KVH, group_size, HD)
    cum_blocks = cum_gate.reshape(KVH, group_size, block_count, block_rows).transpose(2, 0, 1, 3)
    starts = jnp.arange(block_count, dtype=jnp.int32) * block_rows
    key_pos = jnp.arange(length_all, dtype=jnp.int32)

    def attend(bundle):
        query_block, cum_block, offset = bundle
        scores = jnp.einsum('tkgd,skd->kgts', query_block.astype(jnp.float32), keys_wide) * score_factor
        scores = scores + (cum_block[..., None] - cum_keys[:, :, None, :])
        query_pos = offset + jnp.arange(block_rows, dtype=jnp.int32)
        scores = jnp.where(key_pos[None, :] <= query_pos[:, None], scores, -jnp.inf)
        row_max = jnp.max(scores, axis=-1, keepdims=True)
        weights = jnp.exp(scores - row_max)
        totals = jnp.sum(weights, axis=-1)
        rounded = lax.optimization_barrier(weights.astype(jnp.bfloat16)).astype(jnp.float32)
        attended = jnp.einsum('kgts,skd->kgtd', rounded, values_wide) / totals[..., None]
        return attended.astype(jnp.bfloat16).transpose(2, 0, 1, 3).reshape(block_rows, H * HD)

    attended = lax.map(attend, (query_blocks, cum_blocks, starts)).reshape(length_all, H * HD)
    return jnp.dot(attended, w_out, preferred_element_type=jnp.float32).astype(jnp.bfloat16)
```

```python
import functools

import jax
import jax.numpy as jnp
from jax import lax
from jax.experimental import pallas as pl
from jax.experimental.pallas import tpu as pltpu
from jax.sharding import PartitionSpec as P

HD = 64
MESH = pl.DeviceIdType.MESH
CHUNKS = 4


def kernel(
    sp_size, tok, wq, wk, wv, wo, gate, out,
    x, wqv, wboth, wov, gv, kv, qt, top, tot, acc, att, pf, own,
    s_near, s_far, s_own, r_near, r_far, r_own,
    load, tok_s, tok_r, far_s, far_r, fwd_s, fwd_r,
    z_s, x_s, kv_r, o_s, o_r, ready,
    wg, ag, w_s, w_r, a_s, a_r,
):
    f32, bf16 = jnp.float32, jnp.bfloat16
    rows = tok.shape[0]
    half = 2 * rows
    block = 2 * half
    heads = wq.shape[1] // HD
    sp = lax.axis_index("sp")
    t = lax.axis_index("tp")
    core = lax.rem(t, 2)
    p = t // 2
    t1 = t + 1 - 2 * core
    t2 = lax.rem(t + 2, 4)
    t3 = 3 - t
    r = sp // 2
    c = lax.rem(sp, 2)
    last_row = sp_size // 2 - 1
    spx = sp + 1 - 2 * c
    has_next = r < last_row
    pa, pb = p, 1 - p

    def at(n, unit):
        return pl.ds(pl.multiple_of(n * unit, unit), unit)

    loads = [
        pltpu.make_async_copy(tok, x.at[at(t, rows)], load.at[0]),
        pltpu.make_async_copy(gate, gv, load.at[1]),
        pltpu.make_async_copy(wk, wboth.at[0:HD], load.at[2]),
        pltpu.make_async_copy(wv, wboth.at[HD : 2 * HD], load.at[3]),
        pltpu.make_async_copy(wq, wqv, load.at[4]),
        pltpu.make_async_copy(wo, wov, load.at[5]),
    ]
    for copy in loads:
        copy.start()

    barrier = pltpu.get_barrier_semaphore()
    pl.semaphore_signal(barrier, inc=1, device_id={"tp": t1}, device_id_type=MESH)
    pl.semaphore_signal(barrier, inc=1, device_id={"tp": t2}, device_id_type=MESH)
    pl.semaphore_signal(barrier, inc=1, device_id={"tp": t3}, device_id_type=MESH)
    pl.semaphore_signal(barrier, inc=1, device_id={"sp": spx}, device_id_type=MESH)

    @pl.when(has_next)
    def _():
        pl.semaphore_signal(barrier, inc=1, device_id={"sp": sp + 2}, device_id_type=MESH)

    @pl.when(r > 0)
    def _():
        pl.semaphore_signal(barrier, inc=1, device_id={"sp": sp - 2}, device_id_type=MESH)

    peers = 4 + jnp.where(has_next, 1, 0) + jnp.where(r > 0, 1, 0)
    pl.semaphore_wait(barrier, peers)

    step = rows // CHUNKS

    def piece(shard, n):
        return pl.ds(pl.multiple_of(shard * rows + n * step, step), step)

    def remote(src, dst, ss, rs, **where):
        return pltpu.make_async_remote_copy(
            src_ref=src, dst_ref=dst, send_sem=ss, recv_sem=rs,
            device_id=where, device_id_type=MESH,
        )

    far = []
    for n in range(CHUNKS):
        cp = remote(tok.at[pl.ds(n * step, step)], x.at[piece(t, n)], far_s.at[n], far_r.at[n], tp=t2)
        cp.start()
        far.append(cp)
    near = remote(tok, x.at[at(t, rows)], tok_s.at[0], tok_r.at[0], tp=t1)
    near.start()

    loads[1].wait()
    g = gv[...]
    hi = g.astype(bf16).astype(f32)
    mid = (g - hi).astype(bf16).astype(f32)
    low = (g - hi - mid).astype(bf16).astype(f32)
    parts = (hi, mid, low)
    extra = kv.shape[2] - 2 * HD
    index = lax.broadcasted_iota(jnp.int32, (extra, block), 0)
    key_side = jnp.where((index >= 3 * heads) & (index < 3 * heads + 3), 1.0, 0.0).astype(f32)
    for k in range(3):
        for h in range(heads):
            key_side = jnp.where(index == k * heads + h, -parts[k][h : h + 1, :], key_side)
    key_side = key_side.astype(bf16)
    kv[sp, 0, HD : HD + extra, :] = key_side[:, :half]
    kv[sp, 1, HD : HD + extra, :] = key_side[:, half:]
    for h in range(heads):
        side = jnp.where((index < 3 * heads) & (lax.rem(index, heads) == h), 1.0, 0.0).astype(f32)
        for k in range(3):
            side = jnp.where(index == 3 * heads + k, parts[k][h : h + 1, :], side)
        qt[h, HD : HD + extra, :] = side.astype(bf16)

    def project_kv(which):
        xs = x[at(which, half), :]
        both = lax.dot_general(
            wboth[...], xs, (((1,), (1,)), ((), ())), preferred_element_type=f32
        ).astype(bf16)
        kv[sp, which, 0:HD, :] = both[:HD]
        kv[sp, which, HD + extra :, :] = both[HD:]

    def project_q(which):
        xs = x[at(which, half), :]
        q = jnp.dot(xs, wqv[...], preferred_element_type=f32).astype(bf16).astype(f32)
        q = (q * (float(HD) ** -0.5)).T.astype(bf16)
        for h in range(heads):
            qt[h, 0:HD, at(which, half)] = q[h * HD : (h + 1) * HD]

    def along(src, which, row):
        ref = kv.at[src, which]
        return remote(ref, ref, z_s.at[row, which], kv_r.at[src, which], sp=2 * row + c)

    def across(src, which):
        ref = kv.at[src, which]
        return remote(ref, ref, x_s.at[src // 2, which], kv_r.at[src, which], sp=spx)

    def send_own(which):
        @pl.loop(0, last_row - r)
        def _(i):
            along(sp, which, last_row - i).start()

        @pl.when(c == 0)
        def _():
            across(sp, which).start()

    def relay(which):
        @pl.loop(1, r + 1)
        def _(i):
            across(sp - 2 * i, which).wait_recv()
            across(sp - 2 * i, which).start()

    def hear():
        @pl.when(r < last_row - 1)
        def _():
            pl.semaphore_wait(ready, 1)

    @pl.when(r > 0)
    def _():
        hear()

        @pl.when(has_next)
        def _():
            pl.semaphore_signal(ready, inc=1, device_id={"sp": sp - 2}, device_id_type=MESH)

    loads[0].wait()
    loads[2].wait()
    loads[3].wait()
    near.wait_recv()
    project_kv(pa)

    @pl.when(r == 0)
    def _():
        hear()

    send_own(pa)
    loads[4].wait()
    project_q(pa)

    fwd = []
    for n in range(CHUNKS):
        far[n].wait_recv()
        ref = x.at[piece(t2, n)]
        cp = remote(ref, ref, fwd_s.at[n], fwd_r.at[n], tp=t1)
        cp.start()
        fwd.append(cp)

    loads[5].wait()
    split = wo.shape[1] // 2
    gathered = pl.ds(0, split)
    w_far = remote(wov.at[:, gathered], wg.at[t], w_s.at[1], w_r.at[1], tp=t2)
    w_near = remote(wov.at[:, gathered], wg.at[t], w_s.at[0], w_r.at[0], tp=t1)
    w_far.start()

    for n in range(CHUNKS):
        fwd[n].wait_recv()
    w_near.start()
    project_kv(pb)
    send_own(pb)
    relay(pa)
    project_q(pb)

    def attend(src, diagonal):
        kt = jnp.concatenate([kv[src, 0, 0 : HD + extra, :], kv[src, 1, 0 : HD + extra, :]], axis=1)
        vt = jnp.concatenate([kv[src, 0, HD + extra :, :], kv[src, 1, HD + extra :, :]], axis=1)
        for h in range(heads):
            s = lax.dot_general(kt, qt[h], (((0,), (0,)), ((), ())), preferred_element_type=f32)
            lanes = slice(h * HD, (h + 1) * HD)
            if diagonal:
                key_pos = lax.broadcasted_iota(jnp.int32, s.shape, 0)
                query_pos = lax.broadcasted_iota(jnp.int32, s.shape, 1)
                s = jnp.where(key_pos <= query_pos, s, -jnp.inf)
                peak = jnp.max(s, axis=0, keepdims=True)
                w = jnp.exp(s - peak)
                tot[h : h + 1, :] = jnp.sum(w, axis=0, keepdims=True)
                acc[lanes, :] = jnp.dot(vt, w.astype(bf16), preferred_element_type=f32)
            else:
                before = top[h : h + 1, :]
                peak = jnp.maximum(before, jnp.max(s, axis=0, keepdims=True))
                w = jnp.exp(s - peak)
                decay = jnp.exp(before - peak)
                tot[h : h + 1, :] = tot[h : h + 1, :] * decay + jnp.sum(w, axis=0, keepdims=True)
                acc[lanes, :] = acc[lanes, :] * decay + jnp.dot(
                    vt, w.astype(bf16), preferred_element_type=f32
                )
            top[h : h + 1, :] = peak

    attend(sp, True)

    def wait_across(src):
        for which in (pa, pb):
            across(src, which).wait_recv()

    @pl.when(c == 1)
    def _():
        wait_across(spx)
        attend(spx, False)

    relay(pb)

    @pl.loop(1, r + 1)
    def _(i):
        attend(sp - 2 * i, False)

    @pl.loop(1, r + 1)
    def _(i):
        wait_across(spx - 2 * i)
        attend(spx - 2 * i, False)

    for h in range(heads):
        lanes = slice(h * HD, (h + 1) * HD)
        acc[lanes, :] = acc[lanes, :] / tot[h : h + 1, :]
    att[...] = acc[...].T.astype(bf16)
    exchange = []
    for n, peer in ((1, t2), (2, t3), (0, t1)):
        cp = remote(att.at[at(peer, rows)], ag.at[t], a_s.at[n], a_r.at[n], tp=peer)
        cp.start()
        exchange.append(cp)
    width = (wo.shape[1] - split) // CHUNKS
    near_sum, far_sum, own_sum = [], [], []
    for n in range(CHUNKS):
        cols = slice(split + n * width, split + (n + 1) * width)
        pf[:, cols] = jnp.dot(att[at(pb, half), :], wov[:, cols], preferred_element_type=f32)
        s_near[n] = pf[at(1 - core, rows), cols].astype(bf16)
        cp = remote(s_near.at[n], r_near.at[n], o_s.at[0, n], o_r.at[0, n], tp=t1)
        cp.start()
        near_sum.append(cp)
    for n in range(CHUNKS):
        cols = slice(split + n * width, split + (n + 1) * width)
        near_sum[n].wait_recv()
        s_far[n] = (pf[at(core, rows), cols] + r_near[n].astype(f32)).astype(bf16)
        cp = remote(s_far.at[n], r_far.at[n], o_s.at[1, n], o_r.at[1, n], tp=t2)
        cp.start()
        far_sum.append(cp)
    for n in range(CHUNKS):
        cols = slice(split + n * width, split + (n + 1) * width)
        own[:, cols] = jnp.dot(att[at(pa, half), :], wov[:, cols], preferred_element_type=f32)
        s_own[n] = own[at(1 - core, rows), cols].astype(bf16)
        cp = remote(s_own.at[n], r_own.at[n], o_s.at[2, n], o_r.at[2, n], tp=t1)
        cp.start()
        own_sum.append(cp)

    w_far.wait_recv()
    w_fwd = remote(wg.at[t2], wg.at[t2], w_s.at[2], w_r.at[2], tp=t1)
    w_fwd.start()
    total = jnp.dot(att[at(t, rows), :], wov[:, gathered], preferred_element_type=f32)
    for waits, peer in (((w_near, exchange[2]), t1), ((exchange[0],), t2), ((w_fwd, exchange[1]), t3)):
        for cp in waits:
            cp.wait_recv()
        total = total + jnp.dot(ag[peer], wg[peer], preferred_element_type=f32)
    out[:, gathered] = total.astype(bf16)
    for n in range(CHUNKS):
        cols = slice(split + n * width, split + (n + 1) * width)
        own_sum[n].wait_recv()
        far_sum[n].wait_recv()
        total = own[at(core, rows), cols] + r_own[n].astype(f32) + r_far[n].astype(f32)
        out[:, cols] = total.astype(bf16)

    near.wait_send()
    for cp in far + fwd + near_sum + far_sum + own_sum + exchange + [w_far, w_near, w_fwd]:
        cp.wait_send()
    for which in (pa, pb):

        @pl.when(c == 0)
        def _(which=which):
            across(sp, which).wait_send()

        @pl.loop(0, last_row - r)
        def _(i, which=which):
            along(sp, which, last_row - i).wait_send()

        @pl.loop(1, r + 1)
        def _(i, which=which):
            across(sp - 2 * i, which).wait_send()


def per_device(sp_size, tokens, w_query, w_key, w_value, w_out, cum_gate):
    rows, width = tokens.shape
    half, block = 2 * rows, 4 * rows
    heads = w_query.shape[1] // HD
    out_width = w_out.shape[1]
    extra = -(-(3 * heads + 3) // 16) * 16
    bf16, f32 = jnp.bfloat16, jnp.float32
    dma = pltpu.SemaphoreType.DMA
    anywhere = pl.BlockSpec(memory_space=pltpu.HBM)
    part = pltpu.VMEM((CHUNKS, rows, out_width // 2 // CHUNKS), bf16)
    return pl.pallas_call(
        functools.partial(kernel, sp_size),
        out_shape=pltpu.VMEM((rows, out_width), bf16),
        in_specs=[anywhere] * 6,
        out_specs=pl.BlockSpec(memory_space=pltpu.VMEM),
        scratch_shapes=[
            pltpu.VMEM((block, width), bf16),
            pltpu.VMEM(w_query.shape, bf16),
            pltpu.VMEM((2 * HD, width), bf16),
            pltpu.VMEM(w_out.shape, bf16),
            pltpu.VMEM(cum_gate.shape, f32),
            pltpu.VMEM((sp_size, 2, 2 * HD + extra, half), bf16),
            pltpu.VMEM((heads, HD + extra, block), bf16),
            pltpu.VMEM((heads, block), f32),
            pltpu.VMEM((heads, block), f32),
            pltpu.VMEM((heads * HD, block), f32),
            pltpu.VMEM((block, heads * HD), bf16),
            pltpu.VMEM((half, out_width), f32),
            pltpu.VMEM((half, out_width), f32),
            part, part, part, part, part, part,
            dma((6,)),
            dma((1,)), dma((1,)),
            dma((CHUNKS,)), dma((CHUNKS,)),
            dma((CHUNKS,)), dma((CHUNKS,)),
            dma((sp_size // 2, 2)), dma((sp_size // 2, 2)), dma((sp_size, 2)),
            dma((3, CHUNKS)), dma((3, CHUNKS)),
            pltpu.SemaphoreType.REGULAR,
            pltpu.VMEM((4, w_out.shape[0], out_width // 2), bf16),
            pltpu.VMEM((4, rows, w_out.shape[0]), bf16),
            dma((3,)), dma((3,)), dma((3,)), dma((3,)),
        ],
        compiler_params=pltpu.CompilerParams(
            collective_id=0, has_side_effects=True, vmem_limit_bytes=62 * 1024 * 1024
        ),
    )(tokens, w_query, w_key.T, w_value.T, w_out, cum_gate)


def solution(mesh):
    placed = (
        P(("sp", "tp"), None),
        P(None, "tp"),
        P(None, "tp"),
        P(None, "tp"),
        P("tp", None),
        P("tp", "sp"),
    )
    return jax.shard_map(
        functools.partial(per_device, mesh.shape["sp"]),
        mesh=mesh, in_specs=placed, out_specs=P(("sp", "tp"), None), check_vma=False,
    )
```

```python
import functools

import jax
import jax.numpy as jnp
from jax import lax
from jax.experimental import pallas as pl
from jax.experimental.pallas import tpu as pltpu
from jax.sharding import PartitionSpec as P

HD = 64
MESH = pl.DeviceIdType.MESH
CHUNKS = 4
PARTS = 2
FAR = -1e30


def kernel(
    sp_size, tok, wq, wk, wv, wo, gate, out,
    x, wqv, wboth, gv, kv, qt, top, acc, att, part,
    s_far, r_far, wg, ag, ae,
    load, tok_s, tok_r, far_s, far_r, fwd_s, fwd_r,
    z_s, x_s, kv_r, o_s, o_r, ready, w_s, w_r, a_s, a_r,
):
    f32, bf16 = jnp.float32, jnp.bfloat16
    rows = tok.shape[0]
    half = 2 * rows
    block = 2 * half
    heads = wq.shape[1] // HD
    width = wo.shape[1]
    apart = s_far.shape[0] * s_far.shape[2]
    gathered = pl.ds(0, width - apart)
    sp = lax.axis_index("sp")
    t = lax.axis_index("tp")
    core = lax.rem(t, 2)
    p = t // 2
    t1 = t + 1 - 2 * core
    t2 = lax.rem(t + 2, 4)
    t3 = 3 - t
    r = sp // 2
    c = lax.rem(sp, 2)
    last_row = sp_size // 2 - 1
    spx = sp + 1 - 2 * c
    has_next = r < last_row
    pa, pb = p, 1 - p

    def at(n, unit):
        return pl.ds(pl.multiple_of(n * unit, unit), unit)

    loads = [
        pltpu.make_async_copy(tok, x.at[at(t, rows)], load.at[0]),
        pltpu.make_async_copy(gate, gv, load.at[1]),
        pltpu.make_async_copy(wk, wboth.at[0:HD], load.at[2]),
        pltpu.make_async_copy(wv, wboth.at[HD : 2 * HD], load.at[3]),
        pltpu.make_async_copy(wq, wqv, load.at[4]),
        pltpu.make_async_copy(wo, wg.at[t], load.at[5]),
    ]
    for copy in loads:
        copy.start()

    barrier = pltpu.get_barrier_semaphore()
    pl.semaphore_signal(barrier, inc=1, device_id={"tp": t1}, device_id_type=MESH)
    pl.semaphore_signal(barrier, inc=1, device_id={"tp": t2}, device_id_type=MESH)
    pl.semaphore_signal(barrier, inc=1, device_id={"tp": t3}, device_id_type=MESH)
    pl.semaphore_signal(barrier, inc=1, device_id={"sp": spx}, device_id_type=MESH)

    @pl.when(has_next)
    def _():
        pl.semaphore_signal(barrier, inc=1, device_id={"sp": sp + 2}, device_id_type=MESH)

    @pl.when(r > 0)
    def _():
        pl.semaphore_signal(barrier, inc=1, device_id={"sp": sp - 2}, device_id_type=MESH)

    loads[0].wait()
    peers = 4 + jnp.where(has_next, 1, 0) + jnp.where(r > 0, 1, 0)
    pl.semaphore_wait(barrier, peers)

    step = rows // CHUNKS

    def piece(shard, n):
        return pl.ds(pl.multiple_of(shard * rows + n * step, step), step)

    def remote(src, dst, ss, rs, **where):
        return pltpu.make_async_remote_copy(
            src_ref=src, dst_ref=dst, send_sem=ss, recv_sem=rs,
            device_id=where, device_id_type=MESH,
        )

    far = []
    for n in range(CHUNKS):
        ref = x.at[piece(t, n)]
        cp = remote(ref, ref, far_s.at[n], far_r.at[n], tp=t2)
        cp.start()
        far.append(cp)
    mine = x.at[at(t, rows)]
    near = remote(mine, mine, tok_s.at[0], tok_r.at[0], tp=t1)
    near.start()

    loads[1].wait()
    g = gv[...]
    hi = g.astype(bf16).astype(f32)
    mid = (g - hi).astype(bf16).astype(f32)
    low = (g - hi - mid).astype(bf16).astype(f32)
    parts = (hi, mid, low)
    extra = kv.shape[2] - 2 * HD
    index = lax.broadcasted_iota(jnp.int32, (extra, block), 0)
    key_side = jnp.where((index >= 3 * heads) & (index < 3 * heads + 3), 1.0, 0.0).astype(f32)
    for k in range(3):
        for h in range(heads):
            key_side = jnp.where(index == k * heads + h, -parts[k][h : h + 1, :], key_side)
    key_side = key_side.astype(bf16)
    kv[sp, 0, HD : HD + extra, :] = key_side[:, :half]
    kv[sp, 1, HD : HD + extra, :] = key_side[:, half:]
    for h in range(heads):
        side = jnp.where((index < 3 * heads) & (lax.rem(index, heads) == h), 1.0, 0.0).astype(f32)
        for k in range(3):
            side = jnp.where(index == 3 * heads + k, parts[k][h : h + 1, :], side)
        side = side.astype(bf16)
        for which in range(2):
            qt[which, HD : HD + extra, h * half : (h + 1) * half] = side[:, which * half : (which + 1) * half]

    def project_kv(which):
        xs = x[at(which, half), :]
        both = lax.dot_general(
            wboth[...], xs, (((1,), (1,)), ((), ())), preferred_element_type=f32
        ).astype(bf16)
        kv[sp, which, 0:HD, :] = both[:HD]
        kv[sp, which, HD + extra :, :] = both[HD:]

    def project_q(which):
        xs = x[at(which, half), :]
        q = jnp.dot(xs, wqv[...], preferred_element_type=f32).astype(bf16).astype(f32)
        q = (q * (float(HD) ** -0.5)).T.astype(bf16)
        for h in range(heads):
            qt[which, 0:HD, h * half : (h + 1) * half] = q[h * HD : (h + 1) * HD]

    def along(src, which, row):
        ref = kv.at[src, which]
        return remote(ref, ref, z_s.at[row, which], kv_r.at[src, which], sp=2 * row + c)

    def across(src, which):
        ref = kv.at[src, which]
        return remote(ref, ref, x_s.at[src // 2, which], kv_r.at[src, which], sp=spx)

    def send_own(which):
        @pl.loop(0, last_row - r)
        def _(i):
            along(sp, which, last_row - i).start()

        @pl.when(c == 0)
        def _():
            across(sp, which).start()

    def hear():
        @pl.when(r < last_row - 1)
        def _():
            pl.semaphore_wait(ready, 1)

    @pl.when(r > 0)
    def _():
        hear()

        @pl.when(has_next)
        def _():
            pl.semaphore_signal(ready, inc=1, device_id={"sp": sp - 2}, device_id_type=MESH)

    def absorb(*groups, first=False, masked=False):
        scores = []
        for which, pieces in groups:
            q = qt[which]
            for src, kind in pieces:
                s = lax.dot_general(
                    kv[src, kind, 0 : HD + extra, :], q, (((0,), (0,)), ((), ())),
                    preferred_element_type=f32,
                )
                if src is sp and masked:
                    key_pos = lax.broadcasted_iota(jnp.int32, s.shape, 0) + kind * half
                    query_pos = lax.broadcasted_iota(jnp.int32, s.shape, 1) % half + which * half
                    s = jnp.where(key_pos <= query_pos, s, FAR)
                scores.append(s)
        tops, n = [], 0
        for which, pieces in groups:
            peak = None if first else top[which, 0:1, :]
            for _ in pieces:
                high = jnp.max(scores[n], axis=0, keepdims=True)
                peak = high if peak is None else jnp.maximum(peak, high)
                n += 1
            tops.append(peak)
        weights, n = [], 0
        for peak, (which, pieces) in zip(tops, groups):
            for _ in pieces:
                weights.append(jnp.exp(scores[n] - peak).astype(bf16))
                n += 1
        n = 0
        for peak, (which, pieces) in zip(tops, groups):
            total = None
            for src, kind in pieces:
                term = jnp.dot(kv[src, kind, HD:, :], weights[n], preferred_element_type=f32)
                total = term if total is None else total + term
                n += 1
            if not first:
                total = total + acc[which] * jnp.exp(top[which, 0:1, :] - peak)
            acc[which] = total
            top[which, 0:1, :] = peak

    def over(work):
        @pl.loop(0, r // 3)
        def _(j):
            work([3 * j + 1, 3 * j + 2, 3 * j + 3])

        @pl.when(r % 3 == 1)
        def _():
            work([r])

        @pl.when(r % 3 == 2)
        def _():
            work([r - 1, r])

    def forward(n):
        far[n].wait_recv()
        ref = x.at[piece(t2, n)]
        cp = remote(ref, ref, fwd_s.at[n], fwd_r.at[n], tp=t1)
        cp.start()
        return cp

    loads[2].wait()
    loads[3].wait()
    near.wait_recv()
    project_kv(pa)

    @pl.when(r == 0)
    def _():
        hear()

    send_own(pa)
    loads[4].wait()
    project_q(pa)
    loads[5].wait()
    w_near = remote(wg.at[t], wg.at[t], w_s.at[0], w_r.at[0], tp=t1)
    w_near.start()
    absorb((pa, [(sp, pa)]), first=True, masked=True)
    fwd = [forward(0), forward(1)]

    @pl.when(c == 1)
    def _():
        across(spx, pa).wait_recv()
        absorb((pa, [(spx, pa)]))

    def relay(which):
        @pl.loop(1, r + 1)
        def _(i):
            across(sp - 2 * i, which).wait_recv()
            across(sp - 2 * i, which).start()

    relay(pa)
    fwd.append(forward(2))
    w_far = remote(wg.at[t, :, gathered], wg.at[t, :, gathered], w_s.at[1], w_r.at[1], tp=t2)
    w_far.start()
    over(lambda ids: absorb((pa, [(sp - 2 * i, pa) for i in ids])))
    fwd.append(forward(3))
    for cp in fwd:
        cp.wait_recv()
    project_kv(pb)
    send_own(pb)
    project_q(pb)

    @pl.when(c == 0)
    def _():
        absorb((pb, [(sp, pa)]), first=True, masked=True)

    @pl.when(c == 1)
    def _():
        absorb((pb, [(sp, pa), (spx, pa)]), first=True, masked=True)

    def earlier(ids):
        for i in ids:
            across(spx - 2 * i, pa).wait_recv()
        direct = [(sp - 2 * i, pa) for i in ids]
        relayed = [(spx - 2 * i, pa) for i in ids]
        absorb((pb, direct + relayed), (pa, relayed))

    over(earlier)

    @pl.when(c == 0)
    def _():
        absorb((pb, [(sp, pb)]), (pa, [(sp, pb)]), masked=True)

    @pl.when(c == 1)
    def _():
        across(spx, pb).wait_recv()
        both = [(sp, pb), (spx, pb)]
        absorb((pb, both), (pa, both), masked=True)

    relay(pb)

    def directs(ids):
        pieces = [(sp - 2 * i, pb) for i in ids]
        absorb((pb, pieces), (pa, pieces))

    over(directs)

    def lasts(ids):
        for i in ids:
            across(spx - 2 * i, pb).wait_recv()
        absorb((pb, [(spx - 2 * i, pb) for i in ids]))

    over(lasts)

    def settle(which):
        total = acc[which, 3 * heads : 3 * heads + 1, :]
        rest = acc[which, extra : extra + HD, :] / total
        heads_up = jnp.concatenate([rest[:, h * half : (h + 1) * half] for h in range(heads)], axis=0)
        att[which] = heads_up.T.astype(bf16)

    settle(pb)
    theirs, others = att.at[pb, at(core, rows)], att.at[pb, at(1 - core, rows)]
    ex_pair = remote(others, ae, a_s.at[3], a_r.at[3], tp=t1)
    ex_pair.start()
    ex_far = remote(theirs, ag.at[t], a_s.at[1], a_r.at[1], tp=t2)
    ex_far.start()
    ex_skew = remote(others, ag.at[t], a_s.at[2], a_r.at[2], tp=t3)
    ex_skew.start()

    over(lambda ids: absorb((pa, [(spx - 2 * i, pb) for i in ids])))
    w_near.wait_recv()
    ex_pair.wait_recv()
    sums = []
    each = s_far.shape[2]
    for n in range(PARTS):
        cols = slice(width - apart + n * each, width - apart + (n + 1) * each)
        both = jnp.dot(att[pb, at(core, rows), :], wg[t, :, cols], preferred_element_type=f32)
        both += jnp.dot(ae[...], wg[t1, :, cols], preferred_element_type=f32)
        s_far[n] = both.astype(bf16)
        cp = remote(s_far.at[n], r_far.at[n], o_s.at[n], o_r.at[n], tp=t2)
        cp.start()
        sums.append(cp)

    settle(pa)
    ex_near = remote(att.at[pa, at(1 - core, rows)], ag.at[t], a_s.at[0], a_r.at[0], tp=t1)
    ex_near.start()
    w_far.wait_recv()
    w_fwd = remote(wg.at[t2, :, gathered], wg.at[t2, :, gathered], w_s.at[2], w_r.at[2], tp=t1)
    w_fwd.start()
    part[...] = jnp.dot(att[pa, at(core, rows), :], wg[t], preferred_element_type=f32)
    ex_near.wait_recv()
    part[...] += jnp.dot(ag[t1], wg[t1], preferred_element_type=f32)
    ex_far.wait_recv()
    total = part[:, gathered] + jnp.dot(ag[t2], wg[t2, :, gathered], preferred_element_type=f32)
    ex_skew.wait_recv()
    w_fwd.wait_recv()
    total = total + jnp.dot(ag[t3], wg[t3, :, gathered], preferred_element_type=f32)
    out[:, gathered] = total.astype(bf16)
    for n in range(PARTS):
        cols = slice(width - apart + n * each, width - apart + (n + 1) * each)
        sums[n].wait_recv()
        out[:, cols] = (part[:, cols] + r_far[n].astype(f32)).astype(bf16)

    for cp in [near, w_near, w_far, w_fwd, ex_pair, ex_far, ex_skew, ex_near] + far + fwd + sums:
        cp.wait_send()
    for which in (pa, pb):

        @pl.when(c == 0)
        def _(which=which):
            across(sp, which).wait_send()

        @pl.loop(0, last_row - r)
        def _(i, which=which):
            along(sp, which, last_row - i).wait_send()

        @pl.loop(1, r + 1)
        def _(i, which=which):
            across(sp - 2 * i, which).wait_send()


def per_device(sp_size, tokens, w_query, w_key, w_value, w_out, cum_gate):
    rows, width = tokens.shape
    half, block = 2 * rows, 4 * rows
    heads = w_query.shape[1] // HD
    out_width = w_out.shape[1]
    extra = -(-(3 * heads + 3) // 16) * 16
    bf16, f32 = jnp.bfloat16, jnp.float32
    dma = pltpu.SemaphoreType.DMA
    anywhere = pl.BlockSpec(memory_space=pltpu.HBM)
    strip = pltpu.VMEM((PARTS, rows, out_width * 5 // 16), bf16)
    return pl.pallas_call(
        functools.partial(kernel, sp_size),
        out_shape=pltpu.VMEM((rows, out_width), bf16),
        in_specs=[anywhere] * 6,
        out_specs=pl.BlockSpec(memory_space=pltpu.VMEM),
        scratch_shapes=[
            pltpu.VMEM((block, width), bf16),
            pltpu.VMEM(w_query.shape, bf16),
            pltpu.VMEM((2 * HD, width), bf16),
            pltpu.VMEM(cum_gate.shape, f32),
            pltpu.VMEM((sp_size, 2, 2 * HD + extra, half), bf16),
            pltpu.VMEM((2, HD + extra, heads * half), bf16),
            pltpu.VMEM((2, 8, heads * half), f32),
            pltpu.VMEM((2, HD + extra, heads * half), f32),
            pltpu.VMEM((2, half, heads * HD), bf16),
            pltpu.VMEM((rows, out_width), f32),
            strip, strip,
            pltpu.VMEM((4,) + w_out.shape, bf16),
            pltpu.VMEM((4, rows, w_out.shape[0]), bf16),
            pltpu.VMEM((rows, w_out.shape[0]), bf16),
            dma((6,)),
            dma((1,)), dma((1,)),
            dma((CHUNKS,)), dma((CHUNKS,)),
            dma((CHUNKS,)), dma((CHUNKS,)),
            dma((sp_size // 2, 2)), dma((sp_size // 2, 2)), dma((sp_size, 2)),
            dma((PARTS,)), dma((PARTS,)),
            pltpu.SemaphoreType.REGULAR,
            dma((3,)), dma((3,)), dma((4,)), dma((4,)),
        ],
        compiler_params=pltpu.CompilerParams(
            collective_id=0, has_side_effects=True, vmem_limit_bytes=62 * 1024 * 1024
        ),
    )(tokens, w_query, w_key.T, w_value.T, w_out, cum_gate)


def solution(mesh):
    placed = (
        P(("sp", "tp"), None),
        P(None, "tp"),
        P(None, "tp"),
        P(None, "tp"),
        P("tp", None),
        P("tp", "sp"),
    )
    return jax.shard_map(
        functools.partial(per_device, mesh.shape["sp"]),
        mesh=mesh, in_specs=placed, out_specs=P(("sp", "tp"), None), check_vma=False,
    )
```

```python
import functools

import jax
import jax.numpy as jnp
from jax import lax
from jax.experimental import pallas as pl
from jax.experimental.pallas import tpu as pltpu
from jax.sharding import PartitionSpec as P

HD = 64
MESH = pl.DeviceIdType.MESH
CHUNKS = 4
GROUPS = 2
PARTS = 2
FAR = -1e30


def kernel(
    sp_size, tok, wq, wk, wv, wo, gate, out,
    x, wqv, wboth, gv, kv, gk, qt, top, acc, att, part,
    s_far, r_far, wg, ag, ae,
    load, tok_s, tok_r, far_s, far_r, fwd_s, fwd_r,
    z_s, x_s, kv_r, o_s, o_r, ready, w_s, w_r, a_s, a_r,
):
    f32, bf16 = jnp.float32, jnp.bfloat16
    rows = tok.shape[0]
    half = 2 * rows
    block = 2 * half
    heads = wq.shape[1] // HD
    width = wo.shape[1]
    apart = s_far.shape[0] * s_far.shape[2]
    gathered = pl.ds(0, width - apart)
    sp = lax.axis_index("sp")
    t = lax.axis_index("tp")
    core = lax.rem(t, 2)
    p = t // 2
    t1 = t + 1 - 2 * core
    t2 = lax.rem(t + 2, 4)
    t3 = 3 - t
    r = sp // 2
    c = lax.rem(sp, 2)
    last_row = sp_size // 2 - 1
    spx = sp + 1 - 2 * c
    has_next = r < last_row

    def at(n, unit):
        return pl.ds(pl.multiple_of(n * unit, unit), unit)

    span = rows // GROUPS
    loads = [
        pltpu.make_async_copy(gate, gv, load.at[0]),
        pltpu.make_async_copy(wk, wboth.at[0:HD], load.at[1]),
        pltpu.make_async_copy(wv, wboth.at[HD : 2 * HD], load.at[2]),
        pltpu.make_async_copy(wq, wqv, load.at[3]),
        pltpu.make_async_copy(wo, wg.at[t], load.at[4]),
    ]
    arrive = [
        pltpu.make_async_copy(tok.at[pl.ds(n * span, span)], x.at[0, n, core], load.at[5 + n])
        for n in range(GROUPS)
    ]
    for copy in arrive:
        copy.start()
    for copy in loads:
        copy.start()

    barrier = pltpu.get_barrier_semaphore()
    pl.semaphore_signal(barrier, inc=1, device_id={"tp": t1}, device_id_type=MESH)
    pl.semaphore_signal(barrier, inc=1, device_id={"tp": t2}, device_id_type=MESH)
    pl.semaphore_signal(barrier, inc=1, device_id={"tp": t3}, device_id_type=MESH)
    pl.semaphore_signal(barrier, inc=1, device_id={"sp": spx}, device_id_type=MESH)

    @pl.when(has_next)
    def _():
        pl.semaphore_signal(barrier, inc=1, device_id={"sp": sp + 2}, device_id_type=MESH)

    @pl.when(r > 0)
    def _():
        pl.semaphore_signal(barrier, inc=1, device_id={"sp": sp - 2}, device_id_type=MESH)

    for copy in arrive:
        copy.wait()
    peers = 4 + jnp.where(has_next, 1, 0) + jnp.where(r > 0, 1, 0)
    pl.semaphore_wait(barrier, peers)

    step = rows // CHUNKS

    def piece(kind, n):
        return x.at[kind, n * step // span, core, pl.ds(n * step % span, step)]

    def remote(src, dst, ss, rs, **where):
        return pltpu.make_async_remote_copy(
            src_ref=src, dst_ref=dst, send_sem=ss, recv_sem=rs,
            device_id=where, device_id_type=MESH,
        )

    far = []
    for n in range(CHUNKS):
        cp = remote(piece(0, n), piece(1, n), far_s.at[n], far_r.at[n], tp=t2)
        cp.start()
        far.append(cp)
    mine = x.at[0, :, core]
    near = remote(mine, mine, tok_s.at[0], tok_r.at[0], tp=t1)
    near.start()

    def place(n):
        return lax.rem(n // span, 2) * rows + n // (2 * span) * span + lax.rem(n, span)

    loads[0].wait()
    g = gv[...]
    lanes = [slice(core_n * rows + n * span, core_n * rows + (n + 1) * span) for n in range(GROUPS) for core_n in range(2)]
    sides = (jnp.where(p == 0, g[:, :half], g[:, half:]), jnp.where(p == 0, g[:, half:], g[:, :half]))
    extra = (kv.shape[1] - block) // 2
    zeros = jnp.zeros(gk.shape[2:], bf16)
    index = lax.broadcasted_iota(jnp.int32, (extra, half), 0)
    for kind, gs in enumerate(sides):
        gs = jnp.concatenate([gs[:, cut] for cut in lanes], axis=1)
        hi = gs.astype(bf16).astype(f32)
        mid = (gs - hi).astype(bf16).astype(f32)
        low = (gs - hi - mid).astype(bf16).astype(f32)
        parts = (hi, mid, low)
        key_side = jnp.where((index >= 3 * heads) & (index < 3 * heads + 3), 1.0, 0.0).astype(f32)
        for k in range(3):
            for h in range(heads):
                key_side = jnp.where(index == k * heads + h, -parts[k][h : h + 1, :], key_side)
        kv[sp, kind * extra : (kind + 1) * extra, :] = key_side.astype(bf16)
        qt[kind] = jnp.zeros(qt.shape[1:], bf16)
        for h in range(heads):
            side = jnp.where((index < 3 * heads) & (lax.rem(index, heads) == h), 1.0, 0.0).astype(f32)
            for k in range(3):
                side = jnp.where(index == 3 * heads + k, parts[k][h : h + 1, :], side)
            qt[kind, 2 * HD : 2 * HD + extra, h * half : (h + 1) * half] = side.astype(bf16)

    def unpack(src):
        for kind in range(2):
            lines = kv[src, kind * extra : (kind + 1) * extra, :]
            wide = jnp.concatenate([lines, jnp.zeros((gk.shape[2] - extra, half), bf16)], axis=0)
            gk[src, kind * half : (kind + 1) * half, :] = wide.T

    bounds = (0, half, half + half // GROUPS, block)
    lead = 2 * extra

    def project_kv(part_n):
        lo, hi_row = bounds[part_n], bounds[part_n + 1]
        xs = x[0] if part_n == 0 else x[1, part_n - 1]
        both = lax.dot_general(
            xs.reshape(hi_row - lo, x.shape[-1]), wboth[...], (((1,), (1,)), ((), ())),
            preferred_element_type=f32,
        )
        kv[sp, lead + lo : lead + hi_row, :] = both.astype(bf16)

    def project_q(kind):
        xs = x[kind].reshape(half, x.shape[-1])
        q = jnp.dot(xs, wqv[...], preferred_element_type=f32).astype(bf16).astype(f32)
        q = (q * (float(HD) ** -0.5)).T.astype(bf16)
        for h in range(heads):
            qt[kind, 0:HD, h * half : (h + 1) * half] = q[h * HD : (h + 1) * HD]

    def message(src, n):
        return kv.at[src, 0 if n == 0 else lead + bounds[n] : lead + bounds[n + 1]]

    def along(src, n, row):
        ref = message(src, n)
        return remote(ref, ref, z_s.at[row, n], kv_r.at[src, n], sp=2 * row + c)

    def across(src, n):
        ref = message(src, n)
        return remote(ref, ref, x_s.at[src // 2, n], kv_r.at[src, n], sp=spx)

    def send_own(n):
        @pl.loop(0, last_row - r)
        def _(i):
            along(sp, n, last_row - i).start()

        @pl.when(c == 0)
        def _():
            across(sp, n).start()

    def hear():
        @pl.when(r < last_row - 1)
        def _():
            pl.semaphore_wait(ready, 1)

    @pl.when(r > 0)
    def _():
        hear()

        @pl.when(has_next)
        def _():
            pl.semaphore_signal(ready, inc=1, device_id={"sp": sp - 2}, device_id_type=MESH)

    def positions(shape, axis, kind, offset):
        n = lax.rem(lax.broadcasted_iota(jnp.int32, shape, axis), half) + offset
        return place(n) + (p if kind == 0 else 1 - p) * half

    def absorb(*groups, first=()):
        held = {}
        scores = []
        for kind, pieces in groups:
            name = tuple((id(src), lo, hi_row) for src, lo, hi_row in pieces)
            if name not in held:
                keys = jnp.concatenate([kv[src, lead + lo : lead + hi_row, :] for src, lo, hi_row in pieces], axis=0)
                tails = jnp.concatenate([gk[src, lo:hi_row, :] for src, lo, hi_row in pieces], axis=0)
                ones = jnp.ones((16, keys.shape[0]), bf16)
                held[name] = (
                    jnp.concatenate([keys, tails], axis=1),
                    jnp.concatenate([keys.T[HD:], ones], axis=0),
                )
            s = jnp.dot(held[name][0], qt[kind], preferred_element_type=f32)
            cuts, n = [], 0
            for src, lo, hi_row in pieces:
                cut = s[n : n + hi_row - lo]
                n += hi_row - lo
                if src is sp:
                    key_kind = 0 if lo < half else 1
                    key_pos = positions((cut.shape[0], 1), 0, key_kind, lo % half)
                    query_pos = positions((1, cut.shape[1]), 1, kind, 0)
                    cut = jnp.where(key_pos <= query_pos, cut, FAR)
                cuts.append(cut)
            scores.append((name, cuts))
        tops = []
        for (kind, _), (_, cuts) in zip(groups, scores):
            peak = None if kind in first else top[kind, 0:1, :]
            for s in cuts:
                high = jnp.max(s, axis=0, keepdims=True)
                peak = high if peak is None else jnp.maximum(peak, high)
            tops.append(peak)
        weights = [
            jnp.concatenate([jnp.exp(s - peak).astype(bf16) for s in cuts], axis=0)
            for peak, (_, cuts) in zip(tops, scores)
        ]
        for peak, w, (kind, _), (name, _) in zip(tops, weights, groups, scores):
            total = jnp.dot(held[name][1], w, preferred_element_type=f32)
            if kind not in first:
                total = total + acc[kind] * jnp.exp(top[kind, 0:1, :] - peak)
            acc[kind] = total
            top[kind, 0:1, :] = peak

    def over(work):
        @pl.loop(0, r // 3)
        def _(j):
            work([3 * j + 1, 3 * j + 2, 3 * j + 3])

        @pl.when(r % 3 == 1)
        def _():
            work([r])

        @pl.when(r % 3 == 2)
        def _():
            work([r - 1, r])

    def forward(n):
        far[n].wait_recv()
        cp = remote(piece(1, n), piece(1, n), fwd_s.at[n], fwd_r.at[n], tp=t1)
        cp.start()
        return cp

    def relay(n):
        @pl.loop(1, r + 1)
        def _(i):
            across(sp - 2 * i, n).wait_recv()
            across(sp - 2 * i, n).start()

    first_part, early, late, other = [(0, half), (half, bounds[2]), (bounds[2], block), (half, block)]

    loads[1].wait()
    loads[2].wait()
    near.wait_recv()
    project_kv(0)

    @pl.when(r == 0)
    def _():
        hear()

    send_own(0)
    loads[3].wait()
    project_q(0)
    loads[4].wait()
    w_near = remote(wg.at[t], wg.at[t], w_s.at[0], w_r.at[0], tp=t1)
    w_near.start()
    unpack(sp)
    absorb((0, [(sp, *first_part)]), first=(0,))
    fwd = [forward(0), forward(1)]

    @pl.when(c == 1)
    def _():
        across(spx, 0).wait_recv()
        unpack(spx)
        absorb((0, [(spx, *first_part)]))

    relay(0)
    fwd[0].wait_recv()
    fwd[1].wait_recv()
    project_kv(1)
    send_own(1)
    fwd.append(forward(2))
    w_far = remote(wg.at[t, :, gathered], wg.at[t, :, gathered], w_s.at[1], w_r.at[1], tp=t2)
    w_far.start()

    def directs(ids):
        srcs = [sp - 2 * i for i in ids]
        for src in srcs:
            unpack(src)
        absorb((0, [(src, *first_part) for src in srcs]))

    over(directs)
    fwd.append(forward(3))
    absorb((0, [(sp, *early)]))
    fwd[2].wait_recv()
    fwd[3].wait_recv()
    project_kv(2)
    send_own(2)
    project_q(1)
    relay(1)

    @pl.when(c == 0)
    def _():
        absorb((1, [(sp, *first_part), (sp, *other)]), (0, [(sp, *late)]), first=(1,))

    @pl.when(c == 1)
    def _():
        across(spx, 1).wait_recv()
        absorb(
            (1, [(sp, *first_part), (sp, *other), (spx, 0, bounds[2])]),
            (0, [(sp, *late), (spx, *early)]), first=(1,),
        )

    def mixed(ids):
        near_by, beyond = [sp - 2 * i for i in ids], [spx - 2 * i for i in ids]
        for src in beyond:
            across(src, 0).wait_recv()
            unpack(src)
        absorb(
            (1, [(src, 0, bounds[2]) for src in near_by] + [(src, *first_part) for src in beyond]),
            (0, [(src, *early) for src in near_by] + [(src, *first_part) for src in beyond]),
        )

    over(mixed)

    @pl.when(c == 1)
    def _():
        across(spx, 2).wait_recv()
        absorb((1, [(spx, *late)]), (0, [(spx, *late)]))

    relay(2)

    def nearly(ids):
        near_by, beyond = [sp - 2 * i for i in ids], [spx - 2 * i for i in ids]
        for src in beyond:
            across(src, 1).wait_recv()
        pieces = [(src, *late) for src in near_by] + [(src, *early) for src in beyond]
        absorb((1, pieces), (0, pieces))

    over(nearly)

    def lasts(ids):
        beyond = [spx - 2 * i for i in ids]
        for src in beyond:
            across(src, 2).wait_recv()
        absorb((1, [(src, *late) for src in beyond]))

    over(lasts)

    def settle(kind):
        rest = acc[kind, 0:HD, :] / acc[kind, HD : HD + 1, :]
        heads_up = jnp.concatenate([rest[:, h * half : (h + 1) * half] for h in range(heads)], axis=0)
        att[kind] = heads_up.T.astype(bf16).reshape(att.shape[1:])

    settle(1)
    theirs, others = att.at[1, :, core], att.at[1, :, 1 - core]
    ex_pair = remote(others, ae, a_s.at[3], a_r.at[3], tp=t1)
    ex_pair.start()
    ex_far = remote(theirs, ag.at[t], a_s.at[1], a_r.at[1], tp=t2)
    ex_far.start()
    ex_skew = remote(others, ag.at[t], a_s.at[2], a_r.at[2], tp=t3)
    ex_skew.start()
    over(lambda ids: absorb((0, [(spx - 2 * i, *late) for i in ids])))

    def flat(value):
        return value.reshape(rows, value.shape[-1])

    w_near.wait_recv()
    ex_pair.wait_recv()
    sums = []
    each = s_far.shape[2]
    for n in range(PARTS):
        cols = slice(width - apart + n * each, width - apart + (n + 1) * each)
        both = jnp.dot(flat(att[1, :, core]), wg[t, :, cols], preferred_element_type=f32)
        both += jnp.dot(flat(ae[...]), wg[t1, :, cols], preferred_element_type=f32)
        s_far[n] = both.astype(bf16)
        cp = remote(s_far.at[n], r_far.at[n], o_s.at[n], o_r.at[n], tp=t2)
        cp.start()
        sums.append(cp)

    settle(0)
    ex_near = remote(att.at[0, :, 1 - core], ag.at[t], a_s.at[0], a_r.at[0], tp=t1)
    ex_near.start()
    w_far.wait_recv()
    w_fwd = remote(wg.at[t2, :, gathered], wg.at[t2, :, gathered], w_s.at[2], w_r.at[2], tp=t1)
    w_fwd.start()
    part[...] = jnp.dot(flat(att[0, :, core]), wg[t], preferred_element_type=f32)
    ex_near.wait_recv()
    part[...] += jnp.dot(flat(ag[t1]), wg[t1], preferred_element_type=f32)
    ex_far.wait_recv()
    total = part[:, gathered] + jnp.dot(flat(ag[t2]), wg[t2, :, gathered], preferred_element_type=f32)
    ex_skew.wait_recv()
    w_fwd.wait_recv()
    total = total + jnp.dot(flat(ag[t3]), wg[t3, :, gathered], preferred_element_type=f32)
    out[:, gathered] = total.astype(bf16)
    for n in range(PARTS):
        cols = slice(width - apart + n * each, width - apart + (n + 1) * each)
        sums[n].wait_recv()
        out[:, cols] = (part[:, cols] + r_far[n].astype(f32)).astype(bf16)

    for cp in [near, w_near, w_far, w_fwd, ex_pair, ex_far, ex_skew, ex_near] + far + fwd + sums:
        cp.wait_send()
    for which in range(1 + GROUPS):

        @pl.when(c == 0)
        def _(which=which):
            across(sp, which).wait_send()

        @pl.loop(0, last_row - r)
        def _(i, which=which):
            along(sp, which, last_row - i).wait_send()

        @pl.loop(1, r + 1)
        def _(i, which=which):
            across(sp - 2 * i, which).wait_send()


def per_device(sp_size, tokens, w_query, w_key, w_value, w_out, cum_gate):
    rows, width = tokens.shape
    half, block = 2 * rows, 4 * rows
    heads = w_query.shape[1] // HD
    out_width = w_out.shape[1]
    extra = -(-(3 * heads + 3) // 16) * 16
    bf16, f32 = jnp.bfloat16, jnp.float32
    dma = pltpu.SemaphoreType.DMA
    anywhere = pl.BlockSpec(memory_space=pltpu.HBM)
    strip = pltpu.VMEM((PARTS, rows, out_width * 5 // 16), bf16)
    return pl.pallas_call(
        functools.partial(kernel, sp_size),
        out_shape=pltpu.VMEM((rows, out_width), bf16),
        in_specs=[anywhere] * 6,
        out_specs=pl.BlockSpec(memory_space=pltpu.VMEM),
        scratch_shapes=[
            pltpu.VMEM((2, GROUPS, 2, rows // GROUPS, width), bf16),
            pltpu.VMEM(w_query.shape, bf16),
            pltpu.VMEM((2 * HD, width), bf16),
            pltpu.VMEM(cum_gate.shape, f32),
            pltpu.VMEM((sp_size, 2 * extra + block, 2 * HD), bf16),
            pltpu.VMEM((sp_size, block, 2 * HD), bf16),
            pltpu.VMEM((2, 4 * HD, heads * half), bf16),
            pltpu.VMEM((2, 8, heads * half), f32),
            pltpu.VMEM((2, HD + 16, heads * half), f32),
            pltpu.VMEM((2, GROUPS, 2, rows // GROUPS, heads * HD), bf16),
            pltpu.VMEM((rows, out_width), f32),
            strip, strip,
            pltpu.VMEM((4,) + w_out.shape, bf16),
            pltpu.VMEM((4, GROUPS, rows // GROUPS, w_out.shape[0]), bf16),
            pltpu.VMEM((GROUPS, rows // GROUPS, w_out.shape[0]), bf16),
            dma((5 + GROUPS,)),
            dma((1,)), dma((1,)),
            dma((CHUNKS,)), dma((CHUNKS,)),
            dma((CHUNKS,)), dma((CHUNKS,)),
            dma((sp_size // 2, 1 + GROUPS)), dma((sp_size // 2, 1 + GROUPS)), dma((sp_size, 1 + GROUPS)),
            dma((PARTS,)), dma((PARTS,)),
            pltpu.SemaphoreType.REGULAR,
            dma((3,)), dma((3,)), dma((4,)), dma((4,)),
        ],
        compiler_params=pltpu.CompilerParams(
            collective_id=0, has_side_effects=True, vmem_limit_bytes=62 * 1024 * 1024
        ),
    )(tokens, w_query, w_key.T, w_value.T, w_out, cum_gate)


def solution(mesh):
    placed = (
        P(("sp", "tp"), None),
        P(None, "tp"),
        P(None, "tp"),
        P(None, "tp"),
        P("tp", None),
        P("tp", "sp"),
    )
    return jax.shard_map(
        functools.partial(per_device, mesh.shape["sp"]),
        mesh=mesh, in_specs=placed, out_specs=P(("sp", "tp"), None), check_vma=False,
    )
```

```python
import functools

import jax
import jax.numpy as jnp
from jax import lax
from jax.experimental import pallas as pl
from jax.experimental.pallas import tpu as pltpu
from jax.sharding import PartitionSpec as P

HD = 64
MESH = pl.DeviceIdType.MESH
CHUNKS = 4
GROUPS = 2
PARTS = 3
FAR = -1e30


def kernel(
    sp_size, tok, wq, wk, wv, wo, gate, out,
    x, wqv, wboth, gv, kv, gk, qt, top, acc, att, part,
    s_far, r_far, wg, ag, ae,
    load, tok_s, tok_r, far_s, far_r, fwd_s, fwd_r,
    z_s, x_s, kv_r, o_s, o_r, ready, w_s, w_r, a_s, a_r,
):
    f32, bf16 = jnp.float32, jnp.bfloat16
    rows = tok.shape[0]
    half = 2 * rows
    block = 2 * half
    heads = wq.shape[1] // HD
    width = wo.shape[1]
    apart = s_far.shape[0] * s_far.shape[2]
    gathered = pl.ds(0, width - apart)
    sp = lax.axis_index("sp")
    t = lax.axis_index("tp")
    core = lax.rem(t, 2)
    p = t // 2
    t1 = t + 1 - 2 * core
    t2 = lax.rem(t + 2, 4)
    t3 = 3 - t
    r = sp // 2
    c = lax.rem(sp, 2)
    last_row = sp_size // 2 - 1
    spx = sp + 1 - 2 * c
    has_next = r < last_row

    def at(n, unit):
        return pl.ds(pl.multiple_of(n * unit, unit), unit)

    span = rows // GROUPS
    loads = [
        pltpu.make_async_copy(gate, gv, load.at[0]),
        pltpu.make_async_copy(wk, wboth.at[0:HD], load.at[1]),
        pltpu.make_async_copy(wv, wboth.at[HD : 2 * HD], load.at[2]),
        pltpu.make_async_copy(wq, wqv, load.at[3]),
        pltpu.make_async_copy(wo, wg.at[t], load.at[4]),
    ]
    arrive = [
        pltpu.make_async_copy(tok.at[pl.ds(n * span, span)], x.at[0, n, core], load.at[5 + n])
        for n in range(GROUPS)
    ]
    for copy in arrive:
        copy.start()
    for copy in loads:
        copy.start()

    barrier = pltpu.get_barrier_semaphore()
    pl.semaphore_signal(barrier, inc=1, device_id={"tp": t1}, device_id_type=MESH)
    pl.semaphore_signal(barrier, inc=1, device_id={"tp": t2}, device_id_type=MESH)
    pl.semaphore_signal(barrier, inc=1, device_id={"tp": t3}, device_id_type=MESH)
    pl.semaphore_signal(barrier, inc=1, device_id={"sp": spx}, device_id_type=MESH)

    @pl.when(has_next)
    def _():
        pl.semaphore_signal(barrier, inc=1, device_id={"sp": sp + 2}, device_id_type=MESH)

    @pl.when(r > 0)
    def _():
        pl.semaphore_signal(barrier, inc=1, device_id={"sp": sp - 2}, device_id_type=MESH)

    for copy in arrive:
        copy.wait()
    peers = 4 + jnp.where(has_next, 1, 0) + jnp.where(r > 0, 1, 0)
    pl.semaphore_wait(barrier, peers)

    step = rows // CHUNKS

    def piece(kind, n):
        return x.at[kind, n * step // span, core, pl.ds(n * step % span, step)]

    def remote(src, dst, ss, rs, **where):
        return pltpu.make_async_remote_copy(
            src_ref=src, dst_ref=dst, send_sem=ss, recv_sem=rs,
            device_id=where, device_id_type=MESH,
        )

    far = []
    for n in range(CHUNKS):
        cp = remote(piece(0, n), piece(1, n), far_s.at[n], far_r.at[n], tp=t2)
        cp.start()
        far.append(cp)
    mine = x.at[0, :, core]
    near = remote(mine, mine, tok_s.at[0], tok_r.at[0], tp=t1)
    near.start()

    def place(n):
        return lax.rem(n // span, 2) * rows + n // (2 * span) * span + lax.rem(n, span)

    loads[0].wait()
    g = gv[...]
    lanes = [slice(core_n * rows + n * span, core_n * rows + (n + 1) * span) for n in range(GROUPS) for core_n in range(2)]
    sides = (jnp.where(p == 0, g[:, :half], g[:, half:]), jnp.where(p == 0, g[:, half:], g[:, :half]))
    extra = (kv.shape[1] - block) // 2
    zeros = jnp.zeros(gk.shape[2:], bf16)
    index = lax.broadcasted_iota(jnp.int32, (extra, half), 0)
    for kind, gs in enumerate(sides):
        gs = jnp.concatenate([gs[:, cut] for cut in lanes], axis=1)
        hi = gs.astype(bf16).astype(f32)
        mid = (gs - hi).astype(bf16).astype(f32)
        low = (gs - hi - mid).astype(bf16).astype(f32)
        parts = (hi, mid, low)
        key_side = jnp.where((index >= 3 * heads) & (index < 3 * heads + 3), 1.0, 0.0).astype(f32)
        for k in range(3):
            for h in range(heads):
                key_side = jnp.where(index == k * heads + h, -parts[k][h : h + 1, :], key_side)
        kv[sp, kind * extra : (kind + 1) * extra, :] = key_side.astype(bf16)
        qt[kind] = jnp.zeros(qt.shape[1:], bf16)
        for h in range(heads):
            side = jnp.where((index < 3 * heads) & (lax.rem(index, heads) == h), 1.0, 0.0).astype(f32)
            for k in range(3):
                side = jnp.where(index == 3 * heads + k, parts[k][h : h + 1, :], side)
            qt[kind, 2 * HD : 2 * HD + extra, h * half : (h + 1) * half] = side.astype(bf16)

    def unpack(src):
        for kind in range(2):
            lines = kv[src, kind * extra : (kind + 1) * extra, :]
            wide = jnp.concatenate([lines, jnp.zeros((gk.shape[2] - extra, half), bf16)], axis=0)
            gk[src, kind * half : (kind + 1) * half, :] = wide.T

    bounds = (0, half, half + half // GROUPS, block)
    lead = 2 * extra

    def project_kv(part_n):
        lo, hi_row = bounds[part_n], bounds[part_n + 1]
        xs = x[0] if part_n == 0 else x[1, part_n - 1]
        both = lax.dot_general(
            xs.reshape(hi_row - lo, x.shape[-1]), wboth[...], (((1,), (1,)), ((), ())),
            preferred_element_type=f32,
        )
        kv[sp, lead + lo : lead + hi_row, :] = both.astype(bf16)

    def project_q(kind):
        xs = x[kind].reshape(half, x.shape[-1])
        q = jnp.dot(xs, wqv[...], preferred_element_type=f32).astype(bf16).astype(f32)
        q = (q * (float(HD) ** -0.5)).T.astype(bf16)
        for h in range(heads):
            qt[kind, 0:HD, h * half : (h + 1) * half] = q[h * HD : (h + 1) * HD]

    def message(src, n):
        return kv.at[src, 0 if n == 0 else lead + bounds[n] : lead + bounds[n + 1]]

    def along(src, n, row):
        ref = message(src, n)
        return remote(ref, ref, z_s.at[row, n], kv_r.at[src, n], sp=2 * row + c)

    def across(src, n):
        ref = message(src, n)
        return remote(ref, ref, x_s.at[src // 2, n], kv_r.at[src, n], sp=spx)

    def send_own(n):
        @pl.loop(0, last_row - r)
        def _(i):
            along(sp, n, last_row - i).start()

        @pl.when(c == 0)
        def _():
            across(sp, n).start()

    def hear():
        @pl.when(r < last_row - 1)
        def _():
            pl.semaphore_wait(ready, 1)

    @pl.when(r > 0)
    def _():
        hear()

        @pl.when(has_next)
        def _():
            pl.semaphore_signal(ready, inc=1, device_id={"sp": sp - 2}, device_id_type=MESH)

    def positions(shape, axis, kind, offset):
        n = lax.rem(lax.broadcasted_iota(jnp.int32, shape, axis), half) + offset
        return place(n) + (p if kind == 0 else 1 - p) * half

    def absorb(*groups, first=()):
        held = {}
        scores = []
        for kind, pieces in groups:
            name = tuple((id(src), lo, hi_row) for src, lo, hi_row in pieces)
            if name not in held:
                keys = jnp.concatenate([kv[src, lead + lo : lead + hi_row, :] for src, lo, hi_row in pieces], axis=0)
                tails = jnp.concatenate([gk[src, lo:hi_row, :] for src, lo, hi_row in pieces], axis=0)
                ones = jnp.ones((16, keys.shape[0]), bf16)
                held[name] = (
                    jnp.concatenate([keys, tails], axis=1),
                    jnp.concatenate([keys.T[HD:], ones], axis=0),
                )
            s = jnp.dot(held[name][0], qt[kind], preferred_element_type=f32)
            cuts, n = [], 0
            for src, lo, hi_row in pieces:
                cut = s[n : n + hi_row - lo]
                n += hi_row - lo
                if src is sp:
                    key_kind = 0 if lo < half else 1
                    key_pos = positions((cut.shape[0], 1), 0, key_kind, lo % half)
                    query_pos = positions((1, cut.shape[1]), 1, kind, 0)
                    cut = jnp.where(key_pos <= query_pos, cut, FAR)
                cuts.append(cut)
            scores.append((name, cuts))
        tops = []
        for (kind, _), (_, cuts) in zip(groups, scores):
            peak = None if kind in first else top[kind, 0:1, :]
            for s in cuts:
                high = jnp.max(s, axis=0, keepdims=True)
                peak = high if peak is None else jnp.maximum(peak, high)
            tops.append(peak)
        weights = [
            jnp.concatenate([jnp.exp(s - peak).astype(bf16) for s in cuts], axis=0)
            for peak, (_, cuts) in zip(tops, scores)
        ]
        for peak, w, (kind, _), (name, _) in zip(tops, weights, groups, scores):
            total = jnp.dot(held[name][1], w, preferred_element_type=f32)
            if kind not in first:
                total = total + acc[kind] * jnp.exp(top[kind, 0:1, :] - peak)
            acc[kind] = total
            top[kind, 0:1, :] = peak

    def over(work):
        @pl.loop(0, r // 3)
        def _(j):
            work([3 * j + 1, 3 * j + 2, 3 * j + 3])

        @pl.when(r % 3 == 1)
        def _():
            work([r])

        @pl.when(r % 3 == 2)
        def _():
            work([r - 1, r])

    def forward(n):
        far[n].wait_recv()
        cp = remote(piece(1, n), piece(1, n), fwd_s.at[n], fwd_r.at[n], tp=t1)
        cp.start()
        return cp

    def relay(n):
        @pl.loop(1, r + 1)
        def _(i):
            across(sp - 2 * i, n).wait_recv()
            across(sp - 2 * i, n).start()

    first_part, early, late, other = [(0, half), (half, bounds[2]), (bounds[2], block), (half, block)]

    loads[1].wait()
    loads[2].wait()
    near.wait_recv()
    project_kv(0)

    @pl.when(r == 0)
    def _():
        hear()

    send_own(0)
    loads[3].wait()
    project_q(0)
    unpack(sp)
    absorb((0, [(sp, *first_part)]), first=(0,))
    fwd = [forward(0), forward(1)]

    @pl.when(c == 1)
    def _():
        across(spx, 0).wait_recv()
        unpack(spx)
        absorb((0, [(spx, *first_part)]))

    relay(0)
    loads[4].wait()
    w_far = remote(wg.at[t, :, gathered], wg.at[t, :, gathered], w_s.at[1], w_r.at[1], tp=t2)
    w_far.start()
    fwd[0].wait_recv()
    fwd[1].wait_recv()
    project_kv(1)
    send_own(1)
    fwd.append(forward(2))

    def directs(ids):
        srcs = [sp - 2 * i for i in ids]
        for src in srcs:
            unpack(src)
        absorb((0, [(src, *first_part) for src in srcs]))

    over(directs)
    fwd.append(forward(3))
    absorb((0, [(sp, *early)]))
    fwd[2].wait_recv()
    fwd[3].wait_recv()
    project_kv(2)
    send_own(2)
    project_q(1)
    relay(1)

    @pl.when(c == 0)
    def _():
        absorb((1, [(sp, *first_part), (sp, *other)]), (0, [(sp, *late)]), first=(1,))

    @pl.when(c == 1)
    def _():
        across(spx, 1).wait_recv()
        absorb(
            (1, [(sp, *first_part), (sp, *other), (spx, 0, bounds[2])]),
            (0, [(sp, *late), (spx, *early)]), first=(1,),
        )

    def mixed(ids):
        near_by, beyond = [sp - 2 * i for i in ids], [spx - 2 * i for i in ids]
        for src in beyond:
            across(src, 0).wait_recv()
            unpack(src)
        absorb(
            (1, [(src, 0, bounds[2]) for src in near_by] + [(src, *first_part) for src in beyond]),
            (0, [(src, *early) for src in near_by] + [(src, *first_part) for src in beyond]),
        )

    over(mixed)

    @pl.when(c == 1)
    def _():
        across(spx, 2).wait_recv()
        absorb((1, [(spx, *late)]), (0, [(spx, *late)]))

    relay(2)
    w_near = remote(wg.at[t], wg.at[t], w_s.at[0], w_r.at[0], tp=t1)
    w_near.start()

    def nearly(ids):
        near_by, beyond = [sp - 2 * i for i in ids], [spx - 2 * i for i in ids]
        for src in beyond:
            across(src, 1).wait_recv()
        pieces = [(src, *late) for src in near_by] + [(src, *early) for src in beyond]
        absorb((1, pieces), (0, pieces))

    over(nearly)

    def lasts(ids):
        beyond = [spx - 2 * i for i in ids]
        for src in beyond:
            across(src, 2).wait_recv()
        absorb((1, [(src, *late) for src in beyond]))

    over(lasts)

    def settle(kind):
        rest = acc[kind, 0:HD, :] / acc[kind, HD : HD + 1, :]
        heads_up = jnp.concatenate([rest[:, h * half : (h + 1) * half] for h in range(heads)], axis=0)
        att[kind] = heads_up.T.astype(bf16).reshape(att.shape[1:])

    settle(1)
    theirs, others = att.at[1, :, core], att.at[1, :, 1 - core]
    ex_pair = remote(others, ae, a_s.at[3], a_r.at[3], tp=t1)
    ex_pair.start()
    ex_far = remote(theirs, ag.at[t], a_s.at[1], a_r.at[1], tp=t2)
    ex_far.start()
    ex_skew = remote(others, ag.at[t], a_s.at[2], a_r.at[2], tp=t3)
    ex_skew.start()

    def flat(value):
        return value.reshape(rows, value.shape[-1])

    each = s_far.shape[2]

    strips = [slice(width - apart + n * each, width - apart + (n + 1) * each) for n in range(PARTS)]
    for cols in strips:
        part[:, cols] = jnp.dot(flat(att[1, :, core]), wg[t, :, cols], preferred_element_type=f32)
    over(lambda ids: absorb((0, [(spx - 2 * i, *late) for i in ids])))
    w_near.wait_recv()
    ex_pair.wait_recv()
    sums = []
    for n, cols in enumerate(strips):
        both = part[:, cols] + jnp.dot(flat(ae[...]), wg[t1, :, cols], preferred_element_type=f32)
        s_far[n] = both.astype(bf16)
        cp = remote(s_far.at[n], r_far.at[n], o_s.at[n], o_r.at[n], tp=t2)
        cp.start()
        sums.append(cp)

    settle(0)
    ex_near = remote(att.at[0, :, 1 - core], ag.at[t], a_s.at[0], a_r.at[0], tp=t1)
    ex_near.start()
    w_far.wait_recv()
    w_fwd = remote(wg.at[t2, :, gathered], wg.at[t2, :, gathered], w_s.at[2], w_r.at[2], tp=t1)
    w_fwd.start()
    part[...] = jnp.dot(flat(att[0, :, core]), wg[t], preferred_element_type=f32)
    ex_near.wait_recv()
    part[...] += jnp.dot(flat(ag[t1]), wg[t1], preferred_element_type=f32)
    ex_far.wait_recv()
    total = part[:, gathered] + jnp.dot(flat(ag[t2]), wg[t2, :, gathered], preferred_element_type=f32)
    ex_skew.wait_recv()
    w_fwd.wait_recv()
    total = total + jnp.dot(flat(ag[t3]), wg[t3, :, gathered], preferred_element_type=f32)
    out[:, gathered] = total.astype(bf16)
    for n in range(PARTS):
        cols = slice(width - apart + n * each, width - apart + (n + 1) * each)
        sums[n].wait_recv()
        out[:, cols] = (part[:, cols] + r_far[n].astype(f32)).astype(bf16)

    for cp in [near, w_near, w_far, w_fwd, ex_pair, ex_far, ex_skew, ex_near] + far + fwd + sums:
        cp.wait_send()
    for which in range(1 + GROUPS):

        @pl.when(c == 0)
        def _(which=which):
            across(sp, which).wait_send()

        @pl.loop(0, last_row - r)
        def _(i, which=which):
            along(sp, which, last_row - i).wait_send()

        @pl.loop(1, r + 1)
        def _(i, which=which):
            across(sp - 2 * i, which).wait_send()


def per_device(sp_size, tokens, w_query, w_key, w_value, w_out, cum_gate):
    rows, width = tokens.shape
    half, block = 2 * rows, 4 * rows
    heads = w_query.shape[1] // HD
    out_width = w_out.shape[1]
    extra = -(-(3 * heads + 3) // 16) * 16
    bf16, f32 = jnp.bfloat16, jnp.float32
    dma = pltpu.SemaphoreType.DMA
    anywhere = pl.BlockSpec(memory_space=pltpu.HBM)
    strip = pltpu.VMEM((PARTS, rows, out_width * 3 // 16), bf16)
    return pl.pallas_call(
        functools.partial(kernel, sp_size),
        out_shape=pltpu.VMEM((rows, out_width), bf16),
        in_specs=[anywhere] * 6,
        out_specs=pl.BlockSpec(memory_space=pltpu.VMEM),
        scratch_shapes=[
            pltpu.VMEM((2, GROUPS, 2, rows // GROUPS, width), bf16),
            pltpu.VMEM(w_query.shape, bf16),
            pltpu.VMEM((2 * HD, width), bf16),
            pltpu.VMEM(cum_gate.shape, f32),
            pltpu.VMEM((sp_size, 2 * extra + block, 2 * HD), bf16),
            pltpu.VMEM((sp_size, block, 2 * HD), bf16),
            pltpu.VMEM((2, 4 * HD, heads * half), bf16),
            pltpu.VMEM((2, 8, heads * half), f32),
            pltpu.VMEM((2, HD + 16, heads * half), f32),
            pltpu.VMEM((2, GROUPS, 2, rows // GROUPS, heads * HD), bf16),
            pltpu.VMEM((rows, out_width), f32),
            strip, strip,
            pltpu.VMEM((4,) + w_out.shape, bf16),
            pltpu.VMEM((4, GROUPS, rows // GROUPS, w_out.shape[0]), bf16),
            pltpu.VMEM((GROUPS, rows // GROUPS, w_out.shape[0]), bf16),
            dma((5 + GROUPS,)),
            dma((1,)), dma((1,)),
            dma((CHUNKS,)), dma((CHUNKS,)),
            dma((CHUNKS,)), dma((CHUNKS,)),
            dma((sp_size // 2, 1 + GROUPS)), dma((sp_size // 2, 1 + GROUPS)), dma((sp_size, 1 + GROUPS)),
            dma((PARTS,)), dma((PARTS,)),
            pltpu.SemaphoreType.REGULAR,
            dma((3,)), dma((3,)), dma((4,)), dma((4,)),
        ],
        compiler_params=pltpu.CompilerParams(
            collective_id=0, has_side_effects=True, vmem_limit_bytes=62 * 1024 * 1024
        ),
    )(tokens, w_query, w_key.T, w_value.T, w_out, cum_gate)


def solution(mesh):
    placed = (
        P(("sp", "tp"), None),
        P(None, "tp"),
        P(None, "tp"),
        P(None, "tp"),
        P("tp", None),
        P("tp", "sp"),
    )
    return jax.shard_map(
        functools.partial(per_device, mesh.shape["sp"]),
        mesh=mesh, in_specs=placed, out_specs=P(("sp", "tp"), None), check_vma=False,
    )
```

```python
import functools

import jax
import jax.numpy as jnp
from jax import lax
from jax.experimental import pallas as pl
from jax.experimental.pallas import tpu as pltpu
from jax.sharding import PartitionSpec as P

HD = 64
MESH = pl.DeviceIdType.MESH
CHUNKS = 4
GROUPS = 2
SHARED = 4
FAR = -1e30


def kernel(
    sp_size, tok, wq, wk, wv, wo, gate, out,
    x, wqv, wboth, gv, kv, gk, qt, top, acc, att, part,
    s_far, r_far, wg, ag, ae,
    load, tok_s, tok_r, far_s, far_r, fwd_s, fwd_r,
    z_s, x_s, kv_r, o_s, o_r, ready, w_s, w_r, a_s, a_r, y_s, y_r, b_s, b_r, d_s, d_r,
):
    f32, bf16 = jnp.float32, jnp.bfloat16
    rows = tok.shape[0]
    half = 2 * rows
    block = 2 * half
    heads = wq.shape[1] // HD
    width = wo.shape[1]
    apart = s_far.shape[1]
    gathered = pl.ds(0, width - apart)
    unit = width // 16
    alone = pl.ds(2 * SHARED * unit, width - apart - 2 * SHARED * unit)
    sp = lax.axis_index("sp")
    t = lax.axis_index("tp")
    core = lax.rem(t, 2)
    p = t // 2
    t1 = t + 1 - 2 * core
    t2 = lax.rem(t + 2, 4)
    t3 = 3 - t
    r = sp // 2
    c = lax.rem(sp, 2)
    last_row = sp_size // 2 - 1
    spx = sp + 1 - 2 * c
    has_next = r < last_row

    def at(n, unit):
        return pl.ds(pl.multiple_of(n * unit, unit), unit)

    span = rows // GROUPS
    loads = [
        pltpu.make_async_copy(gate, gv, load.at[0]),
        pltpu.make_async_copy(wk, wboth.at[0:HD], load.at[1]),
        pltpu.make_async_copy(wv, wboth.at[HD : 2 * HD], load.at[2]),
        pltpu.make_async_copy(wq, wqv, load.at[3]),
        pltpu.make_async_copy(wo, wg.at[t], load.at[4]),
    ]
    arrive = [
        pltpu.make_async_copy(tok.at[pl.ds(n * span, span)], x.at[0, n, core], load.at[5 + n])
        for n in range(GROUPS)
    ]
    for copy in arrive:
        copy.start()
    for copy in loads:
        copy.start()

    barrier = pltpu.get_barrier_semaphore()
    pl.semaphore_signal(barrier, inc=1, device_id={"tp": t1}, device_id_type=MESH)
    pl.semaphore_signal(barrier, inc=1, device_id={"tp": t2}, device_id_type=MESH)
    pl.semaphore_signal(barrier, inc=1, device_id={"tp": t3}, device_id_type=MESH)
    pl.semaphore_signal(barrier, inc=1, device_id={"sp": spx}, device_id_type=MESH)

    @pl.when(has_next)
    def _():
        pl.semaphore_signal(barrier, inc=1, device_id={"sp": sp + 2}, device_id_type=MESH)

    @pl.when(r > 0)
    def _():
        pl.semaphore_signal(barrier, inc=1, device_id={"sp": sp - 2}, device_id_type=MESH)

    for copy in arrive:
        copy.wait()
    peers = 4 + jnp.where(has_next, 1, 0) + jnp.where(r > 0, 1, 0)
    pl.semaphore_wait(barrier, peers)

    step = rows // CHUNKS

    def piece(kind, n):
        return x.at[kind, n * step // span, core, pl.ds(n * step % span, step)]

    def remote(src, dst, ss, rs, **where):
        return pltpu.make_async_remote_copy(
            src_ref=src, dst_ref=dst, send_sem=ss, recv_sem=rs,
            device_id=where, device_id_type=MESH,
        )

    far = [
        remote(piece(0, n), piece(1, n), far_s.at[n], far_r.at[n], tp=t2) for n in range(CHUNKS)
    ]
    for cp in far[: CHUNKS // GROUPS]:
        cp.start()
    mine = x.at[0, :, core]
    near = remote(mine, mine, tok_s.at[0], tok_r.at[0], tp=t1)
    near.start()

    def place(n):
        return lax.rem(n // span, 2) * rows + n // (2 * span) * span + lax.rem(n, span)

    loads[0].wait()
    g = gv[...]
    lanes = [slice(core_n * rows + n * span, core_n * rows + (n + 1) * span) for n in range(GROUPS) for core_n in range(2)]
    sides = (jnp.where(p == 0, g[:, :half], g[:, half:]), jnp.where(p == 0, g[:, half:], g[:, :half]))
    extra = (kv.shape[1] - block) // 2
    zeros = jnp.zeros(gk.shape[2:], bf16)
    index = lax.broadcasted_iota(jnp.int32, (extra, half), 0)
    for kind, gs in enumerate(sides):
        gs = jnp.concatenate([gs[:, cut] for cut in lanes], axis=1)
        hi = gs.astype(bf16).astype(f32)
        mid = (gs - hi).astype(bf16).astype(f32)
        low = (gs - hi - mid).astype(bf16).astype(f32)
        parts = (hi, mid, low)
        key_side = jnp.where((index >= 3 * heads) & (index < 3 * heads + 3), 1.0, 0.0).astype(f32)
        for k in range(3):
            for h in range(heads):
                key_side = jnp.where(index == k * heads + h, -parts[k][h : h + 1, :], key_side)
        kv[sp, kind * extra : (kind + 1) * extra, :] = key_side.astype(bf16)
        qt[kind] = jnp.zeros(qt.shape[1:], bf16)
        for h in range(heads):
            side = jnp.where((index < 3 * heads) & (lax.rem(index, heads) == h), 1.0, 0.0).astype(f32)
            for k in range(3):
                side = jnp.where(index == 3 * heads + k, parts[k][h : h + 1, :], side)
            qt[kind, 2 * HD : 2 * HD + extra, h * half : (h + 1) * half] = side.astype(bf16)

    def unpack(src):
        for kind in range(2):
            lines = kv[src, kind * extra : (kind + 1) * extra, :]
            wide = jnp.concatenate([lines, jnp.zeros((gk.shape[2] - extra, half), bf16)], axis=0)
            gk[src, kind * half : (kind + 1) * half, :] = wide.T

    bounds = (0, half, half + half // GROUPS, block)
    lead = 2 * extra

    def project_kv(part_n):
        lo, hi_row = bounds[part_n], bounds[part_n + 1]
        xs = x[0] if part_n == 0 else x[1, part_n - 1]
        both = lax.dot_general(
            xs.reshape(hi_row - lo, x.shape[-1]), wboth[...], (((1,), (1,)), ((), ())),
            preferred_element_type=f32,
        )
        kv[sp, lead + lo : lead + hi_row, :] = both.astype(bf16)

    def project_q(kind):
        xs = x[kind].reshape(half, x.shape[-1])
        q = jnp.dot(xs, wqv[...], preferred_element_type=f32).astype(bf16).astype(f32)
        q = (q * (float(HD) ** -0.5)).T.astype(bf16)
        for h in range(heads):
            qt[kind, 0:HD, h * half : (h + 1) * half] = q[h * HD : (h + 1) * HD]

    def message(src, n):
        return kv.at[src, 0 if n == 0 else lead + bounds[n] : lead + bounds[n + 1]]

    def along(src, n, row):
        ref = message(src, n)
        return remote(ref, ref, z_s.at[row, n], kv_r.at[src, n], sp=2 * row + c)

    def across(src, n):
        ref = message(src, n)
        return remote(ref, ref, x_s.at[src // 2, n], kv_r.at[src, n], sp=spx)

    def send_own(n):
        @pl.loop(0, last_row - r)
        def _(i):
            along(sp, n, last_row - i).start()

        @pl.when(c == 0)
        def _():
            across(sp, n).start()

    def hear():
        @pl.when(r < last_row - 1)
        def _():
            pl.semaphore_wait(ready, 1)

    @pl.when(r > 0)
    def _():
        hear()

        @pl.when(has_next)
        def _():
            pl.semaphore_signal(ready, inc=1, device_id={"sp": sp - 2}, device_id_type=MESH)

    def positions(shape, axis, kind, offset):
        n = lax.rem(lax.broadcasted_iota(jnp.int32, shape, axis), half) + offset
        return place(n) + (p if kind == 0 else 1 - p) * half

    def absorb(*groups, first=()):
        held = {}
        scores = []
        for kind, pieces in groups:
            name = tuple((id(src), lo, hi_row) for src, lo, hi_row in pieces)
            if name not in held:
                keys = jnp.concatenate([kv[src, lead + lo : lead + hi_row, :] for src, lo, hi_row in pieces], axis=0)
                tails = jnp.concatenate([gk[src, lo:hi_row, :] for src, lo, hi_row in pieces], axis=0)
                ones = jnp.ones((16, keys.shape[0]), bf16)
                held[name] = (
                    jnp.concatenate([keys, tails], axis=1),
                    jnp.concatenate([keys.T[HD:], ones], axis=0),
                )
            s = jnp.dot(held[name][0], qt[kind], preferred_element_type=f32)
            cuts, n = [], 0
            for src, lo, hi_row in pieces:
                cut = s[n : n + hi_row - lo]
                n += hi_row - lo
                if src is sp:
                    key_kind = 0 if lo < half else 1
                    key_pos = positions((cut.shape[0], 1), 0, key_kind, lo % half)
                    query_pos = positions((1, cut.shape[1]), 1, kind, 0)
                    cut = jnp.where(key_pos <= query_pos, cut, FAR)
                cuts.append(cut)
            scores.append((name, cuts))
        tops = []
        for (kind, _), (_, cuts) in zip(groups, scores):
            peak = None if kind in first else top[kind, 0:1, :]
            for s in cuts:
                high = jnp.max(s, axis=0, keepdims=True)
                peak = high if peak is None else jnp.maximum(peak, high)
            tops.append(peak)
        weights = [
            jnp.concatenate([jnp.exp(s - peak).astype(bf16) for s in cuts], axis=0)
            for peak, (_, cuts) in zip(tops, scores)
        ]
        for peak, w, (kind, _), (name, _) in zip(tops, weights, groups, scores):
            total = jnp.dot(held[name][1], w, preferred_element_type=f32)
            if kind not in first:
                total = total + acc[kind] * jnp.exp(top[kind, 0:1, :] - peak)
            acc[kind] = total
            top[kind, 0:1, :] = peak

    def over(work):
        @pl.loop(0, r // 3)
        def _(j):
            work([3 * j + 1, 3 * j + 2, 3 * j + 3])

        @pl.when(r % 3 == 1)
        def _():
            work([r])

        @pl.when(r % 3 == 2)
        def _():
            work([r - 1, r])

    def strip(k, side):
        return pl.ds(pl.multiple_of((side * SHARED + k) * unit, unit), unit)

    def over_x(k, side):
        ref = wg.at[t2, :, strip(k, side)]
        return remote(ref, ref, b_s.at[k], b_r.at[k], sp=spx)

    def over_chip(k, side, n):
        ref = wg.at[t2, :, strip(k, side)]
        return remote(ref, ref, d_s.at[n, k], d_r.at[n, k], tp=t1)

    def share(k):
        c_far[k].wait_recv()
        over_x(k, c).start()
        over_chip(k, c, 0).start()

    def pass_on(k):
        over_x(k, 1 - c).wait_recv()
        over_chip(k, 1 - c, 1).start()

    def forward(n):
        far[n].wait_recv()
        cp = remote(piece(1, n), piece(1, n), fwd_s.at[n], fwd_r.at[n], tp=t1)
        cp.start()
        return cp

    def relay(n):
        @pl.loop(1, r + 1)
        def _(i):
            across(sp - 2 * i, n).wait_recv()
            across(sp - 2 * i, n).start()

    first_part, early, late, other = [(0, half), (half, bounds[2]), (bounds[2], block), (half, block)]

    loads[1].wait()
    loads[2].wait()
    near.wait_recv()

    @pl.when(core == 0)
    def _():
        for cp in far[CHUNKS // GROUPS :]:
            cp.start()

    project_kv(0)

    @pl.when(r == 0)
    def _():
        hear()

    send_own(0)
    loads[3].wait()
    project_q(0)

    @pl.when(core == 1)
    def _():
        for cp in far[CHUNKS // GROUPS :]:
            cp.start()

    unpack(sp)
    absorb((0, [(sp, *first_part)]), first=(0,))
    fwd = [forward(0), forward(1)]

    @pl.when(c == 1)
    def _():
        across(spx, 0).wait_recv()
        unpack(spx)
        absorb((0, [(spx, *first_part)]))

    relay(0)
    loads[4].wait()
    c_far, w_far = [], remote(wg.at[t, :, alone], wg.at[t, :, alone], w_s.at[1], w_r.at[1], tp=t2)
    for k in range(SHARED):
        ref = wg.at[t, :, strip(k, c)]
        c_far.append(remote(ref, ref, y_s.at[k], y_r.at[k], tp=t2))
        c_far[k].start()
    w_far.start()
    fwd[0].wait_recv()
    fwd[1].wait_recv()
    project_kv(1)
    send_own(1)
    fwd.append(forward(2))

    def directs(ids):
        srcs = [sp - 2 * i for i in ids]
        for src in srcs:
            unpack(src)
        absorb((0, [(src, *first_part) for src in srcs]))

    over(directs)
    fwd.append(forward(3))
    absorb((0, [(sp, *early)]))
    fwd[2].wait_recv()
    fwd[3].wait_recv()
    project_kv(2)
    send_own(2)
    project_q(1)
    relay(1)
    share(0)

    @pl.when(c == 0)
    def _():
        absorb((1, [(sp, *first_part), (sp, *other)]), (0, [(sp, *late)]), first=(1,))

    @pl.when(c == 1)
    def _():
        across(spx, 1).wait_recv()
        absorb(
            (1, [(sp, *first_part), (sp, *other), (spx, 0, bounds[2])]),
            (0, [(sp, *late), (spx, *early)]), first=(1,),
        )

    def mixed(ids):
        near_by, beyond = [sp - 2 * i for i in ids], [spx - 2 * i for i in ids]
        for src in beyond:
            across(src, 0).wait_recv()
            unpack(src)
        absorb(
            (1, [(src, 0, bounds[2]) for src in near_by] + [(src, *first_part) for src in beyond]),
            (0, [(src, *early) for src in near_by] + [(src, *first_part) for src in beyond]),
        )

    over(mixed)

    relay(2)
    w_near = remote(wg.at[t], wg.at[t], w_s.at[0], w_r.at[0], tp=t1)
    w_near.start()
    share(1)

    @pl.when(c == 1)
    def _():
        across(spx, 2).wait_recv()
        absorb((1, [(spx, *late)]), (0, [(spx, *late)]))

    def nearly(ids):
        near_by, beyond = [sp - 2 * i for i in ids], [spx - 2 * i for i in ids]
        for src in beyond:
            across(src, 1).wait_recv()
        pieces = [(src, *late) for src in near_by] + [(src, *early) for src in beyond]
        absorb((1, pieces), (0, pieces))

    over(nearly)
    for k in range(2, SHARED):
        share(k)

    def lasts(ids):
        beyond = [spx - 2 * i for i in ids]
        for src in beyond:
            across(src, 2).wait_recv()
        absorb((1, [(src, *late) for src in beyond]))

    over(lasts)

    def settle(kind):
        rest = acc[kind, 0:HD, :] / acc[kind, HD : HD + 1, :]
        heads_up = jnp.concatenate([rest[:, h * half : (h + 1) * half] for h in range(heads)], axis=0)
        att[kind] = heads_up.T.astype(bf16).reshape(att.shape[1:])

    settle(1)
    theirs, others = att.at[1, :, core], att.at[1, :, 1 - core]
    ex_pair = remote(others, ae, a_s.at[3], a_r.at[3], tp=t1)
    ex_pair.start()
    ex_far = remote(theirs, ag.at[t], a_s.at[1], a_r.at[1], tp=t2)
    ex_far.start()
    ex_skew = remote(others, ag.at[t], a_s.at[2], a_r.at[2], tp=t3)
    ex_skew.start()

    def flat(value):
        return value.reshape(rows, value.shape[-1])

    middle = apart // 256 * 128
    strips = (slice(0, middle), slice(middle, apart))
    rest = slice(width - apart, width)
    part[:, rest] = jnp.dot(flat(att[1, :, core]), wg[t, :, rest], preferred_element_type=f32)
    over(lambda ids: absorb((0, [(spx - 2 * i, *late) for i in ids])))
    w_near.wait_recv()
    ex_pair.wait_recv()
    sums = []
    for n, cut in enumerate(strips):
        cols = slice(width - apart + cut.start, width - apart + cut.stop)
        both = part[:, cols] + jnp.dot(flat(ae[...]), wg[t1, :, cols], preferred_element_type=f32)
        s_far[:, cut] = both.astype(bf16)
        cp = remote(s_far.at[:, cut], r_far.at[:, cut], o_s.at[n], o_r.at[n], tp=t2)
        cp.start()
        sums.append(cp)

    settle(0)
    for k in range(2):
        pass_on(k)
    ex_near = remote(att.at[0, :, 1 - core], ag.at[t], a_s.at[0], a_r.at[0], tp=t1)
    ex_near.start()
    w_far.wait_recv()
    w_fwd = remote(wg.at[t2, :, alone], wg.at[t2, :, alone], w_s.at[2], w_r.at[2], tp=t1)
    w_fwd.start()
    part[...] = jnp.dot(flat(att[0, :, core]), wg[t], preferred_element_type=f32)
    for k in range(2, SHARED):
        pass_on(k)
    ex_near.wait_recv()
    part[...] += jnp.dot(flat(ag[t1]), wg[t1], preferred_element_type=f32)
    ex_far.wait_recv()
    total = part[:, gathered] + jnp.dot(flat(ag[t2]), wg[t2, :, gathered], preferred_element_type=f32)
    ex_skew.wait_recv()
    w_fwd.wait_recv()
    for k in range(SHARED):
        over_chip(k, c, 0).wait_recv()
        over_chip(k, 1 - c, 1).wait_recv()
    total = total + jnp.dot(flat(ag[t3]), wg[t3, :, gathered], preferred_element_type=f32)
    out[:, gathered] = total.astype(bf16)
    for n, cut in enumerate(strips):
        cols = slice(width - apart + cut.start, width - apart + cut.stop)
        sums[n].wait_recv()
        out[:, cols] = (part[:, cols] + r_far[:, cut].astype(f32)).astype(bf16)

    for k in range(SHARED):
        over_x(k, c).wait_send()
        over_chip(k, c, 0).wait_send()
        over_chip(k, 1 - c, 1).wait_send()
    for cp in c_far + [near, w_near, w_far, w_fwd, ex_pair, ex_far, ex_skew, ex_near] + far + fwd + sums:
        cp.wait_send()
    for which in range(1 + GROUPS):

        @pl.when(c == 0)
        def _(which=which):
            across(sp, which).wait_send()

        @pl.loop(0, last_row - r)
        def _(i, which=which):
            along(sp, which, last_row - i).wait_send()

        @pl.loop(1, r + 1)
        def _(i, which=which):
            across(sp - 2 * i, which).wait_send()


def per_device(sp_size, tokens, w_query, w_key, w_value, w_out, cum_gate):
    rows, width = tokens.shape
    half, block = 2 * rows, 4 * rows
    heads = w_query.shape[1] // HD
    out_width = w_out.shape[1]
    extra = -(-(3 * heads + 3) // 16) * 16
    bf16, f32 = jnp.bfloat16, jnp.float32
    dma = pltpu.SemaphoreType.DMA
    anywhere = pl.BlockSpec(memory_space=pltpu.HBM)
    summed = pltpu.VMEM((rows, out_width * 5 // 16), bf16)
    return pl.pallas_call(
        functools.partial(kernel, sp_size),
        out_shape=pltpu.VMEM((rows, out_width), bf16),
        in_specs=[anywhere] * 6,
        out_specs=pl.BlockSpec(memory_space=pltpu.VMEM),
        scratch_shapes=[
            pltpu.VMEM((2, GROUPS, 2, rows // GROUPS, width), bf16),
            pltpu.VMEM(w_query.shape, bf16),
            pltpu.VMEM((2 * HD, width), bf16),
            pltpu.VMEM(cum_gate.shape, f32),
            pltpu.VMEM((sp_size, 2 * extra + block, 2 * HD), bf16),
            pltpu.VMEM((sp_size, block, 2 * HD), bf16),
            pltpu.VMEM((2, 4 * HD, heads * half), bf16),
            pltpu.VMEM((2, 8, heads * half), f32),
            pltpu.VMEM((2, HD + 16, heads * half), f32),
            pltpu.VMEM((2, GROUPS, 2, rows // GROUPS, heads * HD), bf16),
            pltpu.VMEM((rows, out_width), f32),
            summed, summed,
            pltpu.VMEM((4,) + w_out.shape, bf16),
            pltpu.VMEM((4, GROUPS, rows // GROUPS, w_out.shape[0]), bf16),
            pltpu.VMEM((GROUPS, rows // GROUPS, w_out.shape[0]), bf16),
            dma((5 + GROUPS,)),
            dma((1,)), dma((1,)),
            dma((CHUNKS,)), dma((CHUNKS,)),
            dma((CHUNKS,)), dma((CHUNKS,)),
            dma((sp_size // 2, 1 + GROUPS)), dma((sp_size // 2, 1 + GROUPS)), dma((sp_size, 1 + GROUPS)),
            dma((2,)), dma((2,)),
            pltpu.SemaphoreType.REGULAR,
            dma((3,)), dma((3,)), dma((4,)), dma((4,)),
            dma((SHARED,)), dma((SHARED,)), dma((SHARED,)), dma((SHARED,)), dma((2, SHARED)), dma((2, SHARED)),
        ],
        compiler_params=pltpu.CompilerParams(
            collective_id=0, has_side_effects=True, vmem_limit_bytes=62 * 1024 * 1024
        ),
    )(tokens, w_query, w_key.T, w_value.T, w_out, cum_gate)


def solution(mesh):
    placed = (
        P(("sp", "tp"), None),
        P(None, "tp"),
        P(None, "tp"),
        P(None, "tp"),
        P("tp", None),
        P("tp", "sp"),
    )
    return jax.shard_map(
        functools.partial(per_device, mesh.shape["sp"]),
        mesh=mesh, in_specs=placed, out_specs=P(("sp", "tp"), None), check_vma=False,
    )
```

```python
import functools

import jax
import jax.numpy as jnp
from jax import lax
from jax.experimental import pallas as pl
from jax.experimental.pallas import tpu as pltpu
from jax.sharding import PartitionSpec as P

HD = 64
MESH = pl.DeviceIdType.MESH
CHUNKS = 4
GROUPS = 2
SHARED = 4
FAR = -1e30


def kernel(
    sp_size, tok, wq, wk, wv, wo, gate, out,
    x, wqv, wboth, wt, gv, kv, gk, qt, top, acc, att, part,
    s_far, r_far, wg, ag, ae,
    load, tok_s, tok_r, far_s, far_r, fwd_s, fwd_r,
    z_s, x_s, kv_r, o_s, o_r, ready, w_s, w_r, a_s, a_r, y_s, y_r, b_s, b_r, d_s, d_r,
):
    f32, bf16 = jnp.float32, jnp.bfloat16
    rows = tok.shape[0]
    half = 2 * rows
    block = 2 * half
    heads = wq.shape[1] // HD
    width = wo.shape[1]
    apart = s_far.shape[1]
    gathered = pl.ds(0, width - apart)
    unit = width // 16
    alone = pl.ds(2 * SHARED * unit, width - apart - 2 * SHARED * unit)
    sp = lax.axis_index("sp")
    t = lax.axis_index("tp")
    core = lax.rem(t, 2)
    p = t // 2
    t1 = t + 1 - 2 * core
    t2 = lax.rem(t + 2, 4)
    t3 = 3 - t
    r = sp // 2
    c = lax.rem(sp, 2)
    last_row = sp_size // 2 - 1
    spx = sp + 1 - 2 * c
    has_next = r < last_row

    def at(n, unit):
        return pl.ds(pl.multiple_of(n * unit, unit), unit)

    span = rows // GROUPS
    loads = [
        pltpu.make_async_copy(gate, gv, load.at[0]),
        pltpu.make_async_copy(wk, wboth.at[0:HD], load.at[1]),
        pltpu.make_async_copy(wv, wboth.at[HD : 2 * HD], load.at[2]),
        pltpu.make_async_copy(wq, wqv, load.at[3]),
        pltpu.make_async_copy(wo, wg.at[t], load.at[4]),
    ]
    arrive = [
        pltpu.make_async_copy(tok.at[pl.ds(n * span, span)], x.at[0, n, core], load.at[5 + n])
        for n in range(GROUPS)
    ]
    for copy in arrive:
        copy.start()
    for copy in loads:
        copy.start()

    barrier = pltpu.get_barrier_semaphore()
    pl.semaphore_signal(barrier, inc=1, device_id={"tp": t1}, device_id_type=MESH)
    pl.semaphore_signal(barrier, inc=1, device_id={"tp": t2}, device_id_type=MESH)
    pl.semaphore_signal(barrier, inc=1, device_id={"tp": t3}, device_id_type=MESH)
    pl.semaphore_signal(barrier, inc=1, device_id={"sp": spx}, device_id_type=MESH)

    @pl.when(has_next)
    def _():
        pl.semaphore_signal(barrier, inc=1, device_id={"sp": sp + 2}, device_id_type=MESH)

    @pl.when(r > 0)
    def _():
        pl.semaphore_signal(barrier, inc=1, device_id={"sp": sp - 2}, device_id_type=MESH)

    for copy in arrive:
        copy.wait()
    loads[1].wait()
    loads[2].wait()
    wt[...] = wboth[...].T
    peers = 4 + jnp.where(has_next, 1, 0) + jnp.where(r > 0, 1, 0)
    pl.semaphore_wait(barrier, peers)

    step = rows // CHUNKS

    def piece(kind, n):
        return x.at[kind, n * step // span, core, pl.ds(n * step % span, step)]

    def remote(src, dst, ss, rs, **where):
        return pltpu.make_async_remote_copy(
            src_ref=src, dst_ref=dst, send_sem=ss, recv_sem=rs,
            device_id=where, device_id_type=MESH,
        )

    far = [
        remote(piece(0, n), piece(1, n), far_s.at[n], far_r.at[n], tp=t2) for n in range(CHUNKS)
    ]
    for cp in far[: CHUNKS // GROUPS]:
        cp.start()
    mine = x.at[0, :, core]
    near = remote(mine, mine, tok_s.at[0], tok_r.at[0], tp=t1)
    near.start()

    def place(n):
        return lax.rem(n // span, 2) * rows + n // (2 * span) * span + lax.rem(n, span)

    loads[0].wait()
    g = gv[...]
    lanes = [slice(core_n * rows + n * span, core_n * rows + (n + 1) * span) for n in range(GROUPS) for core_n in range(2)]
    sides = (jnp.where(p == 0, g[:, :half], g[:, half:]), jnp.where(p == 0, g[:, half:], g[:, :half]))
    extra = (kv.shape[1] - block) // 2
    zeros = jnp.zeros(gk.shape[2:], bf16)
    index = lax.broadcasted_iota(jnp.int32, (extra, half), 0)
    for kind, gs in enumerate(sides):
        gs = jnp.concatenate([gs[:, cut] for cut in lanes], axis=1)
        hi = gs.astype(bf16).astype(f32)
        mid = (gs - hi).astype(bf16).astype(f32)
        low = (gs - hi - mid).astype(bf16).astype(f32)
        parts = (hi, mid, low)
        key_side = jnp.where((index >= 3 * heads) & (index < 3 * heads + 3), 1.0, 0.0).astype(f32)
        for k in range(3):
            for h in range(heads):
                key_side = jnp.where(index == k * heads + h, -parts[k][h : h + 1, :], key_side)
        kv[sp, kind * extra : (kind + 1) * extra, :] = key_side.astype(bf16)
        qt[kind] = jnp.zeros(qt.shape[1:], bf16)
        for h in range(heads):
            side = jnp.where((index < 3 * heads) & (lax.rem(index, heads) == h), 1.0, 0.0).astype(f32)
            for k in range(3):
                side = jnp.where(index == 3 * heads + k, parts[k][h : h + 1, :], side)
            qt[kind, 2 * HD : 2 * HD + extra, h * half : (h + 1) * half] = side.astype(bf16)

    def unpack(src):
        for kind in range(2):
            lines = kv[src, kind * extra : (kind + 1) * extra, :]
            wide = jnp.concatenate([lines, jnp.zeros((gk.shape[2] - extra, half), bf16)], axis=0)
            gk[src, kind * half : (kind + 1) * half, :] = wide.T

    bounds = (0, half, half + half // GROUPS, block)
    lead = 2 * extra

    def project_kv(part_n):
        lo, hi_row = bounds[part_n], bounds[part_n + 1]
        xs = x[0] if part_n == 0 else x[1, part_n - 1]
        both = jnp.dot(xs.reshape(hi_row - lo, x.shape[-1]), wt[...], preferred_element_type=f32)
        kv[sp, lead + lo : lead + hi_row, :] = both.astype(bf16)

    def project_q(kind):
        xs = x[kind].reshape(half, x.shape[-1])
        q = jnp.dot(xs, wqv[...], preferred_element_type=f32).astype(bf16).astype(f32)
        q = (q * (float(HD) ** -0.5)).T.astype(bf16)
        for h in range(heads):
            qt[kind, 0:HD, h * half : (h + 1) * half] = q[h * HD : (h + 1) * HD]

    def message(src, n):
        return kv.at[src, 0 if n == 0 else lead + bounds[n] : lead + bounds[n + 1]]

    def along(src, n, row):
        ref = message(src, n)
        return remote(ref, ref, z_s.at[row, n], kv_r.at[src, n], sp=2 * row + c)

    def across(src, n):
        ref = message(src, n)
        return remote(ref, ref, x_s.at[src // 2, n], kv_r.at[src, n], sp=spx)

    def send_own(n):
        @pl.loop(0, last_row - r)
        def _(i):
            along(sp, n, last_row - i).start()

        @pl.when(c == 0)
        def _():
            across(sp, n).start()

    def hear():
        @pl.when(r < last_row - 1)
        def _():
            pl.semaphore_wait(ready, 1)

    @pl.when(r > 0)
    def _():
        hear()

        @pl.when(has_next)
        def _():
            pl.semaphore_signal(ready, inc=1, device_id={"sp": sp - 2}, device_id_type=MESH)

    def positions(shape, axis, kind, offset):
        n = lax.rem(lax.broadcasted_iota(jnp.int32, shape, axis), half) + offset
        return place(n) + (p if kind == 0 else 1 - p) * half

    def absorb(*groups, first=()):
        held = {}
        scores = []
        for kind, pieces in groups:
            name = tuple((id(src), lo, hi_row) for src, lo, hi_row in pieces)
            if name not in held:
                keys = jnp.concatenate([kv[src, lead + lo : lead + hi_row, :] for src, lo, hi_row in pieces], axis=0)
                tails = jnp.concatenate([gk[src, lo:hi_row, :] for src, lo, hi_row in pieces], axis=0)
                ones = jnp.ones((16, keys.shape[0]), bf16)
                held[name] = (
                    jnp.concatenate([keys, tails], axis=1),
                    jnp.concatenate([keys.T[HD:], ones], axis=0),
                )
            s = jnp.dot(held[name][0], qt[kind], preferred_element_type=f32)
            cuts, n = [], 0
            for src, lo, hi_row in pieces:
                cut = s[n : n + hi_row - lo]
                n += hi_row - lo
                if src is sp:
                    key_kind = 0 if lo < half else 1
                    key_pos = positions((cut.shape[0], 1), 0, key_kind, lo % half)
                    query_pos = positions((1, cut.shape[1]), 1, kind, 0)
                    cut = jnp.where(key_pos <= query_pos, cut, FAR)
                cuts.append(cut)
            scores.append((name, cuts))
        tops = []
        for (kind, _), (_, cuts) in zip(groups, scores):
            peak = None if kind in first else top[kind, 0:1, :]
            for s in cuts:
                high = jnp.max(s, axis=0, keepdims=True)
                peak = high if peak is None else jnp.maximum(peak, high)
            tops.append(peak)
        weights = [
            jnp.concatenate([jnp.exp(s - peak).astype(bf16) for s in cuts], axis=0)
            for peak, (_, cuts) in zip(tops, scores)
        ]
        for peak, w, (kind, _), (name, _) in zip(tops, weights, groups, scores):
            total = jnp.dot(held[name][1], w, preferred_element_type=f32)
            if kind not in first:
                total = total + acc[kind] * jnp.exp(top[kind, 0:1, :] - peak)
            acc[kind] = total
            top[kind, 0:1, :] = peak

    def over(work):
        @pl.loop(0, r // 3)
        def _(j):
            work([3 * j + 1, 3 * j + 2, 3 * j + 3])

        @pl.when(r % 3 == 1)
        def _():
            work([r])

        @pl.when(r % 3 == 2)
        def _():
            work([r - 1, r])

    def strip(k, side):
        return pl.ds(pl.multiple_of((side * SHARED + k) * unit, unit), unit)

    def over_x(k, side):
        ref = wg.at[t2, :, strip(k, side)]
        return remote(ref, ref, b_s.at[k], b_r.at[k], sp=spx)

    def over_chip(k, side, n):
        ref = wg.at[t2, :, strip(k, side)]
        return remote(ref, ref, d_s.at[n, k], d_r.at[n, k], tp=t1)

    def share(k):
        c_far[k].wait_recv()
        over_x(k, c).start()
        over_chip(k, c, 0).start()

    def pass_on(k):
        over_x(k, 1 - c).wait_recv()
        over_chip(k, 1 - c, 1).start()

    def forward(n):
        far[n].wait_recv()
        cp = remote(piece(1, n), piece(1, n), fwd_s.at[n], fwd_r.at[n], tp=t1)
        cp.start()
        return cp

    def relay(n):
        @pl.loop(1, r + 1)
        def _(i):
            across(sp - 2 * i, n).wait_recv()
            across(sp - 2 * i, n).start()

    first_part, early, late, other = [(0, half), (half, bounds[2]), (bounds[2], block), (half, block)]

    near.wait_recv()

    @pl.when(core == 0)
    def _():
        for cp in far[CHUNKS // GROUPS :]:
            cp.start()

    project_kv(0)

    @pl.when(r == 0)
    def _():
        hear()

    send_own(0)
    loads[3].wait()
    project_q(0)

    @pl.when(core == 1)
    def _():
        for cp in far[CHUNKS // GROUPS :]:
            cp.start()

    unpack(sp)
    absorb((0, [(sp, *first_part)]), first=(0,))
    fwd = [forward(0), forward(1)]

    @pl.when(c == 1)
    def _():
        across(spx, 0).wait_recv()
        unpack(spx)
        absorb((0, [(spx, *first_part)]))

    relay(0)
    loads[4].wait()
    c_far, w_far = [], remote(wg.at[t, :, alone], wg.at[t, :, alone], w_s.at[1], w_r.at[1], tp=t2)
    for k in range(SHARED):
        ref = wg.at[t, :, strip(k, c)]
        c_far.append(remote(ref, ref, y_s.at[k], y_r.at[k], tp=t2))
        c_far[k].start()
    w_far.start()
    fwd[0].wait_recv()
    fwd[1].wait_recv()
    project_kv(1)
    send_own(1)
    fwd.append(forward(2))

    def directs(ids):
        srcs = [sp - 2 * i for i in ids]
        for src in srcs:
            unpack(src)
        absorb((0, [(src, *first_part) for src in srcs]))

    over(directs)
    fwd.append(forward(3))
    absorb((0, [(sp, *early)]))
    fwd[2].wait_recv()
    fwd[3].wait_recv()
    project_kv(2)
    send_own(2)
    project_q(1)
    relay(1)
    share(0)

    @pl.when(c == 0)
    def _():
        absorb((1, [(sp, *first_part), (sp, *other)]), (0, [(sp, *late)]), first=(1,))

    @pl.when(c == 1)
    def _():
        across(spx, 1).wait_recv()
        absorb(
            (1, [(sp, *first_part), (sp, *other), (spx, 0, bounds[2])]),
            (0, [(sp, *late), (spx, *early)]), first=(1,),
        )

    def closer(ids):
        near_by = [sp - 2 * i for i in ids]
        absorb(
            (1, [(src, 0, bounds[2]) for src in near_by]),
            (0, [(src, *early) for src in near_by]),
        )

    over(closer)
    relay(2)
    w_near = remote(wg.at[t], wg.at[t], w_s.at[0], w_r.at[0], tp=t1)
    w_near.start()
    share(1)

    def beyond_x(ids):
        beyond = [spx - 2 * i for i in ids]
        for src in beyond:
            across(src, 0).wait_recv()
            unpack(src)
        pieces = [(src, *first_part) for src in beyond]
        absorb((1, pieces), (0, pieces))

    over(beyond_x)

    @pl.when(c == 1)
    def _():
        across(spx, 2).wait_recv()
        absorb((1, [(spx, *late)]), (0, [(spx, *late)]))

    def nearly(ids):
        near_by, beyond = [sp - 2 * i for i in ids], [spx - 2 * i for i in ids]
        for src in beyond:
            across(src, 1).wait_recv()
        pieces = [(src, *late) for src in near_by] + [(src, *early) for src in beyond]
        absorb((1, pieces), (0, pieces))

    over(nearly)
    for k in range(2, SHARED):
        share(k)

    def lasts(ids):
        beyond = [spx - 2 * i for i in ids]
        for src in beyond:
            across(src, 2).wait_recv()
        absorb((1, [(src, *late) for src in beyond]))

    over(lasts)

    def settle(kind):
        rest = acc[kind, 0:HD, :] / acc[kind, HD : HD + 1, :]
        heads_up = jnp.concatenate([rest[:, h * half : (h + 1) * half] for h in range(heads)], axis=0)
        att[kind] = heads_up.T.astype(bf16).reshape(att.shape[1:])

    settle(1)
    theirs, others = att.at[1, :, core], att.at[1, :, 1 - core]
    ex_pair = remote(others, ae, a_s.at[3], a_r.at[3], tp=t1)
    ex_pair.start()
    ex_far = remote(theirs, ag.at[t], a_s.at[1], a_r.at[1], tp=t2)
    ex_far.start()
    ex_skew = remote(others, ag.at[t], a_s.at[2], a_r.at[2], tp=t3)
    ex_skew.start()

    def flat(value):
        return value.reshape(rows, value.shape[-1])

    middle = apart // 256 * 128
    strips = (slice(0, middle), slice(middle, apart))
    rest = slice(width - apart, width)
    part[:, rest] = jnp.dot(flat(att[1, :, core]), wg[t, :, rest], preferred_element_type=f32)
    over(lambda ids: absorb((0, [(spx - 2 * i, *late) for i in ids])))
    w_near.wait_recv()
    ex_pair.wait_recv()
    sums = []
    for n, cut in enumerate(strips):
        cols = slice(width - apart + cut.start, width - apart + cut.stop)
        both = part[:, cols] + jnp.dot(flat(ae[...]), wg[t1, :, cols], preferred_element_type=f32)
        s_far[:, cut] = both.astype(bf16)
        cp = remote(s_far.at[:, cut], r_far.at[:, cut], o_s.at[n], o_r.at[n], tp=t2)
        cp.start()
        sums.append(cp)

    settle(0)
    for k in range(2):
        pass_on(k)
    ex_near = remote(att.at[0, :, 1 - core], ag.at[t], a_s.at[0], a_r.at[0], tp=t1)
    ex_near.start()
    w_far.wait_recv()
    w_fwd = remote(wg.at[t2, :, alone], wg.at[t2, :, alone], w_s.at[2], w_r.at[2], tp=t1)
    w_fwd.start()
    part[...] = jnp.dot(flat(att[0, :, core]), wg[t], preferred_element_type=f32)
    for k in range(2, SHARED):
        pass_on(k)
    ex_near.wait_recv()
    part[...] += jnp.dot(flat(ag[t1]), wg[t1], preferred_element_type=f32)
    ex_far.wait_recv()
    total = part[:, gathered] + jnp.dot(flat(ag[t2]), wg[t2, :, gathered], preferred_element_type=f32)
    ex_skew.wait_recv()
    w_fwd.wait_recv()
    for k in range(SHARED):
        over_chip(k, c, 0).wait_recv()
        over_chip(k, 1 - c, 1).wait_recv()
    total = total + jnp.dot(flat(ag[t3]), wg[t3, :, gathered], preferred_element_type=f32)
    out[:, gathered] = total.astype(bf16)
    for n, cut in enumerate(strips):
        cols = slice(width - apart + cut.start, width - apart + cut.stop)
        sums[n].wait_recv()
        out[:, cols] = (part[:, cols] + r_far[:, cut].astype(f32)).astype(bf16)

    for k in range(SHARED):
        over_x(k, c).wait_send()
        over_chip(k, c, 0).wait_send()
        over_chip(k, 1 - c, 1).wait_send()
    for cp in c_far + [near, w_near, w_far, w_fwd, ex_pair, ex_far, ex_skew, ex_near] + far + fwd + sums:
        cp.wait_send()
    for which in range(1 + GROUPS):

        @pl.when(c == 0)
        def _(which=which):
            across(sp, which).wait_send()

        @pl.loop(0, last_row - r)
        def _(i, which=which):
            along(sp, which, last_row - i).wait_send()

        @pl.loop(1, r + 1)
        def _(i, which=which):
            across(sp - 2 * i, which).wait_send()


def per_device(sp_size, tokens, w_query, w_key, w_value, w_out, cum_gate):
    rows, width = tokens.shape
    half, block = 2 * rows, 4 * rows
    heads = w_query.shape[1] // HD
    out_width = w_out.shape[1]
    extra = -(-(3 * heads + 3) // 16) * 16
    bf16, f32 = jnp.bfloat16, jnp.float32
    dma = pltpu.SemaphoreType.DMA
    anywhere = pl.BlockSpec(memory_space=pltpu.HBM)
    summed = pltpu.VMEM((rows, out_width * 5 // 16), bf16)
    return pl.pallas_call(
        functools.partial(kernel, sp_size),
        out_shape=pltpu.VMEM((rows, out_width), bf16),
        in_specs=[anywhere] * 6,
        out_specs=pl.BlockSpec(memory_space=pltpu.VMEM),
        scratch_shapes=[
            pltpu.VMEM((2, GROUPS, 2, rows // GROUPS, width), bf16),
            pltpu.VMEM(w_query.shape, bf16),
            pltpu.VMEM((2 * HD, width), bf16),
            pltpu.VMEM((width, 2 * HD), bf16),
            pltpu.VMEM(cum_gate.shape, f32),
            pltpu.VMEM((sp_size, 2 * extra + block, 2 * HD), bf16),
            pltpu.VMEM((sp_size, block, 2 * HD), bf16),
            pltpu.VMEM((2, 4 * HD, heads * half), bf16),
            pltpu.VMEM((2, 8, heads * half), f32),
            pltpu.VMEM((2, HD + 16, heads * half), f32),
            pltpu.VMEM((2, GROUPS, 2, rows // GROUPS, heads * HD), bf16),
            pltpu.VMEM((rows, out_width), f32),
            summed, summed,
            pltpu.VMEM((4,) + w_out.shape, bf16),
            pltpu.VMEM((4, GROUPS, rows // GROUPS, w_out.shape[0]), bf16),
            pltpu.VMEM((GROUPS, rows // GROUPS, w_out.shape[0]), bf16),
            dma((5 + GROUPS,)),
            dma((1,)), dma((1,)),
            dma((CHUNKS,)), dma((CHUNKS,)),
            dma((CHUNKS,)), dma((CHUNKS,)),
            dma((sp_size // 2, 1 + GROUPS)), dma((sp_size // 2, 1 + GROUPS)), dma((sp_size, 1 + GROUPS)),
            dma((2,)), dma((2,)),
            pltpu.SemaphoreType.REGULAR,
            dma((3,)), dma((3,)), dma((4,)), dma((4,)),
            dma((SHARED,)), dma((SHARED,)), dma((SHARED,)), dma((SHARED,)), dma((2, SHARED)), dma((2, SHARED)),
        ],
        compiler_params=pltpu.CompilerParams(
            collective_id=0, has_side_effects=True, vmem_limit_bytes=62 * 1024 * 1024
        ),
    )(tokens, w_query, w_key.T, w_value.T, w_out, cum_gate)


def solution(mesh):
    placed = (
        P(("sp", "tp"), None),
        P(None, "tp"),
        P(None, "tp"),
        P(None, "tp"),
        P("tp", None),
        P("tp", "sp"),
    )
    return jax.shard_map(
        functools.partial(per_device, mesh.shape["sp"]),
        mesh=mesh, in_specs=placed, out_specs=P(("sp", "tp"), None), check_vma=False,
    )
```

```python
import functools

import jax
import jax.numpy as jnp
from jax import lax
from jax.experimental import pallas as pl
from jax.experimental.pallas import tpu as pltpu
from jax.sharding import PartitionSpec as P

HD = 64
MESH = pl.DeviceIdType.MESH
CHUNKS = 4
GROUPS = 2
SHARED = 4
FAR = -1e30


def kernel(
    sp_size, tok, wq, wk, wv, wo, gate, out,
    x, wqv, wboth, wt, gv, kv, gk, qt, top, acc, att, part,
    s_far, r_far, wg, ag, ae,
    load, sent, tok_r, far_r, fwd_r, kv_r, o_r, ready, w_r, a_r, y_r, b_r, d_r,
):
    f32, bf16 = jnp.float32, jnp.bfloat16
    rows = tok.shape[0]
    half = 2 * rows
    block = 2 * half
    heads = wq.shape[1] // HD
    width = wo.shape[1]
    apart = r_far.shape[1]
    gathered = pl.ds(0, width - apart)
    unit = width // 16
    alone = pl.ds(2 * SHARED * unit, width - apart - 2 * SHARED * unit)
    sp = lax.axis_index("sp")
    t = lax.axis_index("tp")
    core = lax.rem(t, 2)
    p = t // 2
    t1 = t + 1 - 2 * core
    t2 = lax.rem(t + 2, 4)
    t3 = 3 - t
    r = sp // 2
    c = lax.rem(sp, 2)
    last_row = sp_size // 2 - 1
    spx = sp + 1 - 2 * c
    has_next = r < last_row

    def at(n, unit):
        return pl.ds(pl.multiple_of(n * unit, unit), unit)

    span = rows // GROUPS
    loads = [
        pltpu.make_async_copy(gate, gv, load.at[0]),
        pltpu.make_async_copy(wk, wboth.at[0:HD], load.at[1]),
        pltpu.make_async_copy(wv, wboth.at[HD : 2 * HD], load.at[1]),
        pltpu.make_async_copy(wq, wqv, load.at[2]),
        pltpu.make_async_copy(wo, wg.at[t], load.at[3]),
    ]
    arrive = [
        pltpu.make_async_copy(tok.at[pl.ds(n * span, span)], x.at[0, n, core], load.at[4])
        for n in range(GROUPS)
    ]
    for copy in arrive:
        copy.start()
    for copy in loads:
        copy.start()

    def drain(ref, semaphore):
        pltpu.make_async_copy(ref, ref, semaphore).wait()

    barrier = pltpu.get_barrier_semaphore()
    pl.semaphore_signal(barrier, inc=1, device_id={"tp": t1}, device_id_type=MESH)
    pl.semaphore_signal(barrier, inc=1, device_id={"tp": t2}, device_id_type=MESH)
    pl.semaphore_signal(barrier, inc=1, device_id={"tp": t3}, device_id_type=MESH)
    pl.semaphore_signal(barrier, inc=1, device_id={"sp": spx}, device_id_type=MESH)

    @pl.when(has_next)
    def _():
        pl.semaphore_signal(barrier, inc=1, device_id={"sp": sp + 2}, device_id_type=MESH)

    @pl.when(r > 0)
    def _():
        pl.semaphore_signal(barrier, inc=1, device_id={"sp": sp - 2}, device_id_type=MESH)

    drain(x.at[0, :, core], load.at[4])
    drain(wboth, load.at[1])
    wt[...] = wboth[...].T
    peers = 4 + jnp.where(has_next, 1, 0) + jnp.where(r > 0, 1, 0)
    pl.semaphore_wait(barrier, peers)

    step = rows // CHUNKS

    def piece(kind, n):
        return x.at[kind, n * step // span, core, pl.ds(n * step % span, step)]

    def remote(src, dst, ss, rs, **where):
        return pltpu.make_async_remote_copy(
            src_ref=src, dst_ref=dst, send_sem=ss, recv_sem=rs,
            device_id=where, device_id_type=MESH,
        )

    far = [
        remote(piece(0, n), piece(1, n), sent.at[0], far_r.at[n], tp=t2) for n in range(CHUNKS)
    ]
    for cp in far[: CHUNKS // GROUPS]:
        cp.start()
    mine = x.at[0, :, core]
    near = remote(mine, mine, sent.at[0], tok_r.at[0], tp=t1)
    near.start()

    def place(n):
        return lax.rem(n // span, 2) * rows + n // (2 * span) * span + lax.rem(n, span)

    loads[0].wait()
    g = gv[...]
    lanes = [slice(core_n * rows + n * span, core_n * rows + (n + 1) * span) for n in range(GROUPS) for core_n in range(2)]
    sides = (jnp.where(p == 0, g[:, :half], g[:, half:]), jnp.where(p == 0, g[:, half:], g[:, :half]))
    extra = (kv.shape[1] - block) // 2
    zeros = jnp.zeros(gk.shape[2:], bf16)
    index = lax.broadcasted_iota(jnp.int32, (extra, half), 0)
    for kind, gs in enumerate(sides):
        gs = jnp.concatenate([gs[:, cut] for cut in lanes], axis=1)
        hi = gs.astype(bf16).astype(f32)
        mid = (gs - hi).astype(bf16).astype(f32)
        low = (gs - hi - mid).astype(bf16).astype(f32)
        parts = (hi, mid, low)
        key_side = jnp.where((index >= 3 * heads) & (index < 3 * heads + 3), 1.0, 0.0).astype(f32)
        for k in range(3):
            for h in range(heads):
                key_side = jnp.where(index == k * heads + h, -parts[k][h : h + 1, :], key_side)
        kv[sp, kind * extra : (kind + 1) * extra, :] = key_side.astype(bf16)
        qt[kind] = jnp.zeros(qt.shape[1:], bf16)
        for h in range(heads):
            side = jnp.where((index < 3 * heads) & (lax.rem(index, heads) == h), 1.0, 0.0).astype(f32)
            for k in range(3):
                side = jnp.where(index == 3 * heads + k, parts[k][h : h + 1, :], side)
            qt[kind, 2 * HD : 2 * HD + extra, h * half : (h + 1) * half] = side.astype(bf16)

    def unpack(src):
        for kind in range(2):
            lines = kv[src, kind * extra : (kind + 1) * extra, :]
            wide = jnp.concatenate([lines, jnp.zeros((gk.shape[2] - extra, half), bf16)], axis=0)
            gk[src, kind * half : (kind + 1) * half, :] = wide.T

    bounds = (0, half, half + half // GROUPS, block)
    lead = 2 * extra

    def project_kv(part_n):
        lo, hi_row = bounds[part_n], bounds[part_n + 1]
        xs = x[0] if part_n == 0 else x[1, part_n - 1]
        both = jnp.dot(xs.reshape(hi_row - lo, x.shape[-1]), wt[...], preferred_element_type=f32)
        kv[sp, lead + lo : lead + hi_row, :] = both.astype(bf16)

    def project_q(kind):
        xs = x[kind].reshape(half, x.shape[-1])
        q = jnp.dot(xs, wqv[...], preferred_element_type=f32).astype(bf16).astype(f32)
        q = (q * (float(HD) ** -0.5)).T.astype(bf16)
        for h in range(heads):
            qt[kind, 0:HD, h * half : (h + 1) * half] = q[h * HD : (h + 1) * HD]

    def message(src, n):
        return kv.at[src, 0 if n == 0 else lead + bounds[n] : lead + bounds[n + 1]]

    def along(src, n, row):
        ref = message(src, n)
        return remote(ref, ref, sent.at[1], kv_r.at[src, n], sp=2 * row + c)

    def across(src, n):
        ref = message(src, n)
        return remote(ref, ref, sent.at[1], kv_r.at[src, n], sp=spx)

    def send_own(n):
        @pl.loop(0, last_row - r)
        def _(i):
            along(sp, n, last_row - i).start()

        @pl.when(c == 0)
        def _():
            across(sp, n).start()

    def hear():
        @pl.when(r < last_row - 1)
        def _():
            pl.semaphore_wait(ready, 1)

    @pl.when(r > 0)
    def _():
        hear()

        @pl.when(has_next)
        def _():
            pl.semaphore_signal(ready, inc=1, device_id={"sp": sp - 2}, device_id_type=MESH)

    def positions(shape, axis, kind, offset):
        n = lax.rem(lax.broadcasted_iota(jnp.int32, shape, axis), half) + offset
        return place(n) + (p if kind == 0 else 1 - p) * half

    def absorb(*groups, first=()):
        held = {}
        scores = []
        for kind, pieces in groups:
            name = tuple((id(src), lo, hi_row) for src, lo, hi_row in pieces)
            if name not in held:
                keys = jnp.concatenate([kv[src, lead + lo : lead + hi_row, :] for src, lo, hi_row in pieces], axis=0)
                tails = jnp.concatenate([gk[src, lo:hi_row, :] for src, lo, hi_row in pieces], axis=0)
                ones = jnp.ones((16, keys.shape[0]), bf16)
                held[name] = (
                    jnp.concatenate([keys, tails], axis=1),
                    jnp.concatenate([keys.T[HD:], ones], axis=0),
                )
            s = jnp.dot(held[name][0], qt[kind], preferred_element_type=f32)
            cuts, n = [], 0
            for src, lo, hi_row in pieces:
                cut = s[n : n + hi_row - lo]
                n += hi_row - lo
                if src is sp:
                    key_kind = 0 if lo < half else 1
                    key_pos = positions((cut.shape[0], 1), 0, key_kind, lo % half)
                    query_pos = positions((1, cut.shape[1]), 1, kind, 0)
                    cut = jnp.where(key_pos <= query_pos, cut, FAR)
                cuts.append(cut)
            scores.append((name, cuts))
        tops = []
        for (kind, _), (_, cuts) in zip(groups, scores):
            peak = None if kind in first else top[kind, 0:1, :]
            for s in cuts:
                high = jnp.max(s, axis=0, keepdims=True)
                peak = high if peak is None else jnp.maximum(peak, high)
            tops.append(peak)
        weights = [
            jnp.concatenate([jnp.exp(s - peak).astype(bf16) for s in cuts], axis=0)
            for peak, (_, cuts) in zip(tops, scores)
        ]
        for peak, w, (kind, _), (name, _) in zip(tops, weights, groups, scores):
            total = jnp.dot(held[name][1], w, preferred_element_type=f32)
            if kind not in first:
                total = total + acc[kind] * jnp.exp(top[kind, 0:1, :] - peak)
            acc[kind] = total
            top[kind, 0:1, :] = peak

    def over(work):
        @pl.loop(0, r // 3)
        def _(j):
            work([3 * j + 1, 3 * j + 2, 3 * j + 3])

        @pl.when(r % 3 == 1)
        def _():
            work([r])

        @pl.when(r % 3 == 2)
        def _():
            work([r - 1, r])

    def strip(k, side):
        return pl.ds(pl.multiple_of((side * SHARED + k) * unit, unit), unit)

    def over_x(k, side):
        ref = wg.at[t2, :, strip(k, side)]
        return remote(ref, ref, sent.at[2], b_r.at[k], sp=spx)

    def over_chip(k, side, n):
        ref = wg.at[t2, :, strip(k, side)]
        return remote(ref, ref, sent.at[2], d_r, tp=t1)

    def share(k):
        c_far[k].wait_recv()
        over_x(k, c).start()
        over_chip(k, c, 0).start()

    def pass_on(k):
        over_x(k, 1 - c).wait_recv()
        over_chip(k, 1 - c, 1).start()

    def forward(n):
        far[n].wait_recv()
        cp = remote(piece(1, n), piece(1, n), sent.at[0], fwd_r.at[n * step // span], tp=t1)
        cp.start()
        return cp

    def relay(n):
        @pl.loop(1, r + 1)
        def _(i):
            across(sp - 2 * i, n).wait_recv()
            across(sp - 2 * i, n).start()

    first_part, early, late, other = [(0, half), (half, bounds[2]), (bounds[2], block), (half, block)]

    near.wait_recv()

    @pl.when(core == 0)
    def _():
        for cp in far[CHUNKS // GROUPS :]:
            cp.start()

    project_kv(0)

    @pl.when(r == 0)
    def _():
        hear()

    send_own(0)
    loads[3].wait()
    project_q(0)

    @pl.when(core == 1)
    def _():
        for cp in far[CHUNKS // GROUPS :]:
            cp.start()

    unpack(sp)
    absorb((0, [(sp, *first_part)]), first=(0,))
    fwd = [forward(0), forward(1)]

    @pl.when(c == 1)
    def _():
        across(spx, 0).wait_recv()
        unpack(spx)
        absorb((0, [(spx, *first_part)]))

    relay(0)
    loads[4].wait()
    c_far, w_far = [], remote(wg.at[t, :, alone], wg.at[t, :, alone], sent.at[4], w_r.at[1], tp=t2)
    for k in range(SHARED):
        ref = wg.at[t, :, strip(k, c)]
        c_far.append(remote(ref, ref, sent.at[2], y_r.at[k], tp=t2))
        c_far[k].start()
    w_far.start()
    drain(x.at[1, 0, 1 - core], fwd_r.at[0])
    project_kv(1)
    send_own(1)
    fwd.append(forward(2))

    def directs(ids):
        srcs = [sp - 2 * i for i in ids]
        for src in srcs:
            unpack(src)
        absorb((0, [(src, *first_part) for src in srcs]))

    over(directs)
    fwd.append(forward(3))
    absorb((0, [(sp, *early)]))
    drain(x.at[1, 1, 1 - core], fwd_r.at[1])
    project_kv(2)
    send_own(2)
    project_q(1)
    relay(1)
    share(0)

    @pl.when(c == 0)
    def _():
        absorb((1, [(sp, *first_part), (sp, *other)]), (0, [(sp, *late)]), first=(1,))

    @pl.when(c == 1)
    def _():
        across(spx, 1).wait_recv()
        absorb(
            (1, [(sp, *first_part), (sp, *other), (spx, 0, bounds[2])]),
            (0, [(sp, *late), (spx, *early)]), first=(1,),
        )

    def closer(ids):
        near_by = [sp - 2 * i for i in ids]
        absorb(
            (1, [(src, 0, bounds[2]) for src in near_by]),
            (0, [(src, *early) for src in near_by]),
        )

    over(closer)
    relay(2)
    w_near = remote(wg.at[t], wg.at[t], sent.at[3], w_r.at[0], tp=t1)
    w_near.start()
    share(1)

    def beyond_x(ids):
        beyond = [spx - 2 * i for i in ids]
        for src in beyond:
            across(src, 0).wait_recv()
            unpack(src)
        pieces = [(src, *first_part) for src in beyond]
        absorb((1, pieces), (0, pieces))

    over(beyond_x)

    @pl.when(c == 1)
    def _():
        across(spx, 2).wait_recv()
        absorb((1, [(spx, *late)]), (0, [(spx, *late)]))

    def nearly(ids):
        near_by, beyond = [sp - 2 * i for i in ids], [spx - 2 * i for i in ids]
        for src in beyond:
            across(src, 1).wait_recv()
        pieces = [(src, *late) for src in near_by] + [(src, *early) for src in beyond]
        absorb((1, pieces), (0, pieces))

    over(nearly)
    for k in range(2, SHARED):
        share(k)

    def lasts(ids):
        beyond = [spx - 2 * i for i in ids]
        for src in beyond:
            across(src, 2).wait_recv()
        absorb((1, [(src, *late) for src in beyond]))

    over(lasts)

    def settle(kind):
        rest = acc[kind, 0:HD, :] / acc[kind, HD : HD + 1, :]
        heads_up = jnp.concatenate([rest[:, h * half : (h + 1) * half] for h in range(heads)], axis=0)
        att[kind] = heads_up.T.astype(bf16).reshape(att.shape[1:])

    settle(1)
    theirs, others = att.at[1, :, core], att.at[1, :, 1 - core]
    ex_far = remote(theirs, ag.at[t], sent.at[5], a_r.at[1], tp=t2)
    ex_far.start()
    ex_skew = remote(others, ag.at[t], sent.at[5], a_r.at[2], tp=t3)
    ex_skew.start()

    def flat(value):
        return value.reshape(rows, value.shape[-1])

    middle = apart // 256 * 128
    strips = (slice(0, middle), slice(middle, apart))
    ex_pair = remote(att.at[1], ae, sent.at[6], a_r.at[3], tp=t1)

    def sums(n, side):
        to = t2 if side == 0 else t3
        cut = strips[n]
        return remote(s_far.at[side, :, cut], r_far.at[:, cut], sent.at[6], o_r.at[n], tp=to)

    w_near.wait_recv()

    @pl.when(core == 1)
    def _():
        ex_pair.start()

    @pl.when(core == 0)
    def _():
        ex_pair.wait_recv()
        for n, cut in enumerate(strips):
            cols = slice(width - apart + cut.start, width - apart + cut.stop)
            both = jnp.dot(att[1].reshape(half, -1), wg[t, :, cols], preferred_element_type=f32)
            both = both + jnp.dot(ae[...].reshape(half, -1), wg[t1, :, cols], preferred_element_type=f32)
            both = both.astype(bf16).reshape(GROUPS, 2, span, -1)
            for side in range(2):
                s_far[side, :, cut] = both[:, side].reshape(rows, -1)
                sums(n, side).start()

    over(lambda ids: absorb((0, [(spx - 2 * i, *late) for i in ids])))
    settle(0)
    for k in range(2):
        pass_on(k)
    ex_near = remote(att.at[0, :, 1 - core], ag.at[t], sent.at[5], a_r.at[0], tp=t1)
    ex_near.start()
    w_far.wait_recv()
    w_fwd = remote(wg.at[t2, :, alone], wg.at[t2, :, alone], sent.at[4], w_r.at[2], tp=t1)
    w_fwd.start()
    part[...] = jnp.dot(flat(att[0, :, core]), wg[t], preferred_element_type=f32)
    for k in range(2, SHARED):
        pass_on(k)
    ex_near.wait_recv()
    part[...] += jnp.dot(flat(ag[t1]), wg[t1], preferred_element_type=f32)
    ex_far.wait_recv()
    total = part[:, gathered] + jnp.dot(flat(ag[t2]), wg[t2, :, gathered], preferred_element_type=f32)
    ex_skew.wait_recv()
    w_fwd.wait_recv()
    drain(wg.at[0, :, : 2 * SHARED * unit], d_r)
    total = total + jnp.dot(flat(ag[t3]), wg[t3, :, gathered], preferred_element_type=f32)
    out[:, gathered] = total.astype(bf16)
    drain(wg.at[0:3, 0:rows], sent.at[0])

    @pl.when(c == 0)
    def _():
        drain(kv.at[0 : last_row + 1], sent.at[1])

    @pl.when(c == 1)
    def _():
        drain(kv.at[0:last_row], sent.at[1])

    drain(wg.at[0, :, : 4 * SHARED * unit], sent.at[2])
    w_near.wait_send()
    drain(wg.at[0, :, : 2 * alone.size], sent.at[4])
    drain(ag.at[0:3], sent.at[5])

    for n, cut in enumerate(strips):
        cols = slice(width - apart + cut.start, width - apart + cut.stop)
        sums(n, 0).wait_recv()
        out[:, cols] = (part[:, cols] + r_far[:, cut].astype(f32)).astype(bf16)

    @pl.when(core == 1)
    def _():
        ex_pair.wait_send()

    @pl.when(core == 0)
    def _():
        drain(s_far, sent.at[6])


def per_device(sp_size, tokens, w_query, w_key, w_value, w_out, cum_gate):
    rows, width = tokens.shape
    half, block = 2 * rows, 4 * rows
    heads = w_query.shape[1] // HD
    out_width = w_out.shape[1]
    extra = -(-(3 * heads + 3) // 16) * 16
    bf16, f32 = jnp.bfloat16, jnp.float32
    dma = pltpu.SemaphoreType.DMA
    anywhere = pl.BlockSpec(memory_space=pltpu.HBM)
    summed = (rows, out_width * 5 // 16)
    return pl.pallas_call(
        functools.partial(kernel, sp_size),
        out_shape=pltpu.VMEM((rows, out_width), bf16),
        in_specs=[anywhere] * 6,
        out_specs=pl.BlockSpec(memory_space=pltpu.VMEM),
        scratch_shapes=[
            pltpu.VMEM((2, GROUPS, 2, rows // GROUPS, width), bf16),
            pltpu.VMEM(w_query.shape, bf16),
            pltpu.VMEM((2 * HD, width), bf16),
            pltpu.VMEM((width, 2 * HD), bf16),
            pltpu.VMEM(cum_gate.shape, f32),
            pltpu.VMEM((sp_size, 2 * extra + block, 2 * HD), bf16),
            pltpu.VMEM((sp_size, block, 2 * HD), bf16),
            pltpu.VMEM((2, 4 * HD, heads * half), bf16),
            pltpu.VMEM((2, 8, heads * half), f32),
            pltpu.VMEM((2, HD + 16, heads * half), f32),
            pltpu.VMEM((2, GROUPS, 2, rows // GROUPS, heads * HD), bf16),
            pltpu.VMEM((rows, out_width), f32),
            pltpu.VMEM((2,) + summed, bf16), pltpu.VMEM(summed, bf16),
            pltpu.VMEM((4,) + w_out.shape, bf16),
            pltpu.VMEM((4, GROUPS, rows // GROUPS, w_out.shape[0]), bf16),
            pltpu.VMEM((GROUPS, 2, rows // GROUPS, w_out.shape[0]), bf16),
            dma((5,)), dma((7,)), dma((1,)), dma((CHUNKS,)), dma((GROUPS,)),
            dma((sp_size, 1 + GROUPS)), dma((2,)), pltpu.SemaphoreType.REGULAR,
            dma((3,)), dma((4,)), dma((SHARED,)), dma((SHARED,)), dma(()),
        ],
        compiler_params=pltpu.CompilerParams(
            collective_id=0, has_side_effects=True, vmem_limit_bytes=62 * 1024 * 1024
        ),
    )(tokens, w_query, w_key.T, w_value.T, w_out, cum_gate)


def solution(mesh):
    placed = (
        P(("sp", "tp"), None),
        P(None, "tp"),
        P(None, "tp"),
        P(None, "tp"),
        P("tp", None),
        P("tp", "sp"),
    )
    return jax.shard_map(
        functools.partial(per_device, mesh.shape["sp"]),
        mesh=mesh, in_specs=placed, out_specs=P(("sp", "tp"), None), check_vma=False,
    )
```

```python
import functools

import jax
import jax.numpy as jnp
from jax import lax
from jax.experimental import pallas as pl
from jax.experimental.pallas import tpu as pltpu
from jax.sharding import PartitionSpec as P

HD = 64
MESH = pl.DeviceIdType.MESH
CHUNKS = 4
GROUPS = 2
SHARED = 4
FAR = -1e30


def kernel(
    sp_size, tok, wq, wk, wv, wo, gate, out,
    x, wqv, wboth, wt, gv, kv, gk, qt, top, acc, att, part,
    s_far, r_far, wg, ag, ae,
    load, sent, tok_r, far_r, fwd_r, kv_r, o_r, ready, w_r, a_r, y_r, b_r, d_r,
):
    f32, bf16 = jnp.float32, jnp.bfloat16
    rows = tok.shape[0]
    half = 2 * rows
    block = 2 * half
    heads = wq.shape[1] // HD
    width = wo.shape[1]
    apart = r_far.shape[1]
    gathered = pl.ds(0, width - apart)
    unit = width // 16
    alone = pl.ds(2 * SHARED * unit, width - apart - 2 * SHARED * unit)
    sp = lax.axis_index("sp")
    t = lax.axis_index("tp")
    core = lax.rem(t, 2)
    p = t // 2
    t1 = t + 1 - 2 * core
    t2 = lax.rem(t + 2, 4)
    t3 = 3 - t
    r = sp // 2
    c = lax.rem(sp, 2)
    last_row = sp_size // 2 - 1
    spx = sp + 1 - 2 * c
    has_next = r < last_row

    def at(n, unit):
        return pl.ds(pl.multiple_of(n * unit, unit), unit)

    span = rows // GROUPS
    loads = [
        pltpu.make_async_copy(gate, gv, load.at[0]),
        pltpu.make_async_copy(wk, wboth.at[0:HD], load.at[1]),
        pltpu.make_async_copy(wv, wboth.at[HD : 2 * HD], load.at[1]),
        pltpu.make_async_copy(wq, wqv, load.at[2]),
        pltpu.make_async_copy(wo, wg.at[t], load.at[3]),
    ]
    arrive = [
        pltpu.make_async_copy(tok.at[pl.ds(n * span, span)], x.at[0, n, core], load.at[4])
        for n in range(GROUPS)
    ]
    for copy in arrive:
        copy.start()
    for copy in loads:
        copy.start()

    def drain(ref, semaphore):
        pltpu.make_async_copy(ref, ref, semaphore).wait()

    barrier = pltpu.get_barrier_semaphore()
    pl.semaphore_signal(barrier, inc=1, device_id={"tp": t1}, device_id_type=MESH)
    pl.semaphore_signal(barrier, inc=1, device_id={"tp": t2}, device_id_type=MESH)
    pl.semaphore_signal(barrier, inc=1, device_id={"tp": t3}, device_id_type=MESH)
    pl.semaphore_signal(barrier, inc=1, device_id={"sp": spx}, device_id_type=MESH)

    @pl.when(has_next)
    def _():
        pl.semaphore_signal(barrier, inc=1, device_id={"sp": sp + 2}, device_id_type=MESH)

    @pl.when(r > 0)
    def _():
        pl.semaphore_signal(barrier, inc=1, device_id={"sp": sp - 2}, device_id_type=MESH)

    drain(x.at[0, :, core], load.at[4])
    drain(wboth, load.at[1])
    wt[...] = wboth[...].T
    peers = 4 + jnp.where(has_next, 1, 0) + jnp.where(r > 0, 1, 0)
    pl.semaphore_wait(barrier, peers)

    step = rows // CHUNKS

    def piece(kind, n):
        return x.at[kind, n * step // span, core, pl.ds(n * step % span, step)]

    def remote(src, dst, ss, rs, **where):
        return pltpu.make_async_remote_copy(
            src_ref=src, dst_ref=dst, send_sem=ss, recv_sem=rs,
            device_id=where, device_id_type=MESH,
        )

    far = [
        remote(piece(0, n), piece(1, n), sent.at[0], far_r.at[n], tp=t2) for n in range(CHUNKS)
    ]
    for cp in far[: CHUNKS // GROUPS]:
        cp.start()
    mine = x.at[0, :, core]
    near = remote(mine, mine, sent.at[0], tok_r.at[0], tp=t1)
    near.start()

    def place(n):
        return lax.rem(n // span, 2) * rows + n // (2 * span) * span + lax.rem(n, span)

    loads[0].wait()
    g = gv[...]
    lanes = [slice(core_n * rows + n * span, core_n * rows + (n + 1) * span) for n in range(GROUPS) for core_n in range(2)]
    sides = (jnp.where(p == 0, g[:, :half], g[:, half:]), jnp.where(p == 0, g[:, half:], g[:, :half]))
    extra = (kv.shape[1] - block) // 2
    zeros = jnp.zeros(gk.shape[2:], bf16)
    index = lax.broadcasted_iota(jnp.int32, (extra, half), 0)
    for kind, gs in enumerate(sides):
        gs = jnp.concatenate([gs[:, cut] for cut in lanes], axis=1)
        hi = gs.astype(bf16).astype(f32)
        mid = (gs - hi).astype(bf16).astype(f32)
        low = (gs - hi - mid).astype(bf16).astype(f32)
        parts = (hi, mid, low)
        key_side = jnp.where((index >= 3 * heads) & (index < 3 * heads + 3), 1.0, 0.0).astype(f32)
        for k in range(3):
            for h in range(heads):
                key_side = jnp.where(index == k * heads + h, -parts[k][h : h + 1, :], key_side)
        kv[sp, kind * extra : (kind + 1) * extra, :] = key_side.astype(bf16)
        qt[kind] = jnp.zeros(qt.shape[1:], bf16)
        for h in range(heads):
            side = jnp.where((index < 3 * heads) & (lax.rem(index, heads) == h), 1.0, 0.0).astype(f32)
            for k in range(3):
                side = jnp.where(index == 3 * heads + k, parts[k][h : h + 1, :], side)
            qt[kind, 2 * HD : 2 * HD + extra, h * half : (h + 1) * half] = side.astype(bf16)

    def unpack(src):
        for kind in range(2):
            lines = kv[src, kind * extra : (kind + 1) * extra, :]
            wide = jnp.concatenate([lines, jnp.zeros((gk.shape[2] - extra, half), bf16)], axis=0)
            gk[src, kind * half : (kind + 1) * half, :] = wide.T

    bounds = (0, half, half + half // GROUPS, block)
    lead = 2 * extra

    def project_kv(part_n):
        lo, hi_row = bounds[part_n], bounds[part_n + 1]
        xs = x[0] if part_n == 0 else x[1, part_n - 1]
        both = jnp.dot(xs.reshape(hi_row - lo, x.shape[-1]), wt[...], preferred_element_type=f32)
        kv[sp, lead + lo : lead + hi_row, :] = both.astype(bf16)

    def project_q(kind):
        xs = x[kind].reshape(half, x.shape[-1])
        q = jnp.dot(xs, wqv[...], preferred_element_type=f32).astype(bf16).astype(f32)
        q = (q * (float(HD) ** -0.5)).T.astype(bf16)
        for h in range(heads):
            qt[kind, 0:HD, h * half : (h + 1) * half] = q[h * HD : (h + 1) * HD]

    def message(src, n):
        return kv.at[src, 0 if n == 0 else lead + bounds[n] : lead + bounds[n + 1]]

    def along(src, n, row):
        ref = message(src, n)
        return remote(ref, ref, sent.at[1], kv_r.at[src, n], sp=2 * row + c)

    def across(src, n):
        ref = message(src, n)
        return remote(ref, ref, sent.at[1], kv_r.at[src, n], sp=spx)

    def send_own(n):
        @pl.loop(0, last_row - r)
        def _(i):
            along(sp, n, last_row - i).start()

        @pl.when(c == 0)
        def _():
            across(sp, n).start()

    def hear():
        @pl.when(r < last_row - 1)
        def _():
            pl.semaphore_wait(ready, 1)

    @pl.when(r > 0)
    def _():
        hear()

        @pl.when(has_next)
        def _():
            pl.semaphore_signal(ready, inc=1, device_id={"sp": sp - 2}, device_id_type=MESH)

    def positions(shape, axis, kind, offset):
        n = lax.rem(lax.broadcasted_iota(jnp.int32, shape, axis), half) + offset
        return place(n) + (p if kind == 0 else 1 - p) * half

    def absorb(*groups, first=()):
        held = {}
        scores = []
        for kind, pieces in groups:
            name = tuple((id(src), lo, hi_row) for src, lo, hi_row in pieces)
            if name not in held:
                keys = jnp.concatenate([kv[src, lead + lo : lead + hi_row, :] for src, lo, hi_row in pieces], axis=0)
                tails = jnp.concatenate([gk[src, lo:hi_row, :] for src, lo, hi_row in pieces], axis=0)
                ones = jnp.ones((16, keys.shape[0]), bf16)
                held[name] = (
                    jnp.concatenate([keys, tails], axis=1),
                    jnp.concatenate([keys.T[HD:], ones], axis=0),
                )
            s = jnp.dot(held[name][0], qt[kind], preferred_element_type=f32)
            cuts, n = [], 0
            for src, lo, hi_row in pieces:
                cut = s[n : n + hi_row - lo]
                n += hi_row - lo
                if src is sp:
                    key_kind = 0 if lo < half else 1
                    key_pos = positions((cut.shape[0], 1), 0, key_kind, lo % half)
                    query_pos = positions((1, cut.shape[1]), 1, kind, 0)
                    cut = jnp.where(key_pos <= query_pos, cut, FAR)
                cuts.append(cut)
            scores.append((name, cuts))
        tops = []
        for (kind, _), (_, cuts) in zip(groups, scores):
            peak = None if kind in first else top[kind, 0:1, :]
            for s in cuts:
                high = jnp.max(s, axis=0, keepdims=True)
                peak = high if peak is None else jnp.maximum(peak, high)
            tops.append(peak)
        weights = [
            jnp.concatenate([jnp.exp(s - peak).astype(bf16) for s in cuts], axis=0)
            for peak, (_, cuts) in zip(tops, scores)
        ]
        for peak, w, (kind, _), (name, _) in zip(tops, weights, groups, scores):
            total = jnp.dot(held[name][1], w, preferred_element_type=f32)
            if kind not in first:
                total = total + acc[kind] * jnp.exp(top[kind, 0:1, :] - peak)
            acc[kind] = total
            top[kind, 0:1, :] = peak

    def over(work):
        @pl.loop(0, r // 3)
        def _(j):
            work([3 * j + 1, 3 * j + 2, 3 * j + 3])

        @pl.when(r % 3 == 1)
        def _():
            work([r])

        @pl.when(r % 3 == 2)
        def _():
            work([r - 1, r])

    def strip(k, side):
        return pl.ds(pl.multiple_of((side * SHARED + k) * unit, unit), unit)

    def over_x(k, side):
        ref = wg.at[t2, :, strip(k, side)]
        return remote(ref, ref, sent.at[2], b_r.at[k], sp=spx)

    def over_chip(k, side, n):
        ref = wg.at[t2, :, strip(k, side)]
        return remote(ref, ref, sent.at[2], d_r, tp=t1)

    def share(k):
        c_far[k].wait_recv()
        over_x(k, c).start()
        over_chip(k, c, 0).start()

    def pass_on(k):
        over_x(k, 1 - c).wait_recv()
        over_chip(k, 1 - c, 1).start()

    def forward(n):
        far[n].wait_recv()
        cp = remote(piece(1, n), piece(1, n), sent.at[0], fwd_r.at[n * step // span], tp=t1)
        cp.start()
        return cp

    def relay(n):
        @pl.loop(1, r + 1)
        def _(i):
            across(sp - 2 * i, n).wait_recv()
            across(sp - 2 * i, n).start()

    first_part, early, late, other = [(0, half), (half, bounds[2]), (bounds[2], block), (half, block)]

    near.wait_recv()

    @pl.when(core == 0)
    def _():
        for cp in far[CHUNKS // GROUPS :]:
            cp.start()

    project_kv(0)

    @pl.when(r == 0)
    def _():
        hear()

    send_own(0)
    loads[3].wait()
    project_q(0)

    @pl.when(core == 1)
    def _():
        for cp in far[CHUNKS // GROUPS :]:
            cp.start()

    unpack(sp)
    absorb((0, [(sp, *first_part)]), first=(0,))
    fwd = [forward(0), forward(1)]

    @pl.when(c == 1)
    def _():
        across(spx, 0).wait_recv()
        unpack(spx)
        absorb((0, [(spx, *first_part)]))

    relay(0)
    loads[4].wait()
    c_far, w_far = [], remote(wg.at[t, :, alone], wg.at[t, :, alone], sent.at[4], w_r.at[1], tp=t2)
    for k in range(SHARED):
        ref = wg.at[t, :, strip(k, c)]
        c_far.append(remote(ref, ref, sent.at[2], y_r.at[k], tp=t2))
        c_far[k].start()
    w_far.start()
    drain(x.at[1, 0, 1 - core], fwd_r.at[0])
    project_kv(1)
    send_own(1)
    fwd.append(forward(2))

    def directs(ids):
        srcs = [sp - 2 * i for i in ids]
        for src in srcs:
            unpack(src)
        absorb((0, [(src, *first_part) for src in srcs]))

    over(directs)
    fwd.append(forward(3))
    absorb((0, [(sp, *early)]))
    drain(x.at[1, 1, 1 - core], fwd_r.at[1])
    project_kv(2)
    send_own(2)
    project_q(1)
    relay(1)

    @pl.when(core == 1)
    def _():
        share(0)

    @pl.when(c == 0)
    def _():
        absorb((1, [(sp, *first_part), (sp, *other)]), (0, [(sp, *late)]), first=(1,))

    @pl.when(c == 1)
    def _():
        across(spx, 1).wait_recv()
        absorb(
            (1, [(sp, *first_part), (sp, *other), (spx, 0, bounds[2])]),
            (0, [(sp, *late), (spx, *early)]), first=(1,),
        )

    def closer(ids):
        near_by = [sp - 2 * i for i in ids]
        absorb(
            (1, [(src, 0, bounds[2]) for src in near_by]),
            (0, [(src, *early) for src in near_by]),
        )

    over(closer)
    relay(2)
    w_near = remote(wg.at[t], wg.at[t], sent.at[3], w_r.at[0], tp=t1)
    w_near.start()

    @pl.when(core == 0)
    def _():
        share(0)

    share(1)

    def beyond_x(ids):
        beyond = [spx - 2 * i for i in ids]
        for src in beyond:
            across(src, 0).wait_recv()
            unpack(src)
        pieces = [(src, *first_part) for src in beyond]
        absorb((1, pieces), (0, pieces))

    over(beyond_x)

    @pl.when(c == 1)
    def _():
        across(spx, 2).wait_recv()
        absorb((1, [(spx, *late)]), (0, [(spx, *late)]))

    def nearly(ids):
        near_by, beyond = [sp - 2 * i for i in ids], [spx - 2 * i for i in ids]
        for src in beyond:
            across(src, 1).wait_recv()
        pieces = [(src, *late) for src in near_by] + [(src, *early) for src in beyond]
        absorb((1, pieces), (0, pieces))

    over(nearly)
    for k in range(2, SHARED):
        share(k)

    def lasts(ids):
        beyond = [spx - 2 * i for i in ids]
        for src in beyond:
            across(src, 2).wait_recv()
        absorb((1, [(src, *late) for src in beyond]))

    over(lasts)

    def settle(kind):
        rest = acc[kind, 0:HD, :] / acc[kind, HD : HD + 1, :]
        heads_up = jnp.concatenate([rest[:, h * half : (h + 1) * half] for h in range(heads)], axis=0)
        att[kind] = heads_up.T.astype(bf16).reshape(att.shape[1:])

    settle(1)
    theirs, others = att.at[1, :, core], att.at[1, :, 1 - core]
    ex_far = remote(theirs, ag.at[t], sent.at[5], a_r.at[1], tp=t2)
    ex_far.start()
    ex_skew = remote(others, ag.at[t], sent.at[5], a_r.at[2], tp=t3)
    ex_skew.start()

    def flat(value):
        return value.reshape(rows, value.shape[-1])

    middle = apart // 256 * 128
    strips = (slice(0, middle), slice(middle, apart))
    ex_pair = remote(att.at[1], ae, sent.at[6], a_r.at[3], tp=t1)

    def sums(n, side):
        to = t2 if side == 0 else t3
        cut = strips[n]
        return remote(s_far.at[side, :, cut], r_far.at[:, cut], sent.at[6], o_r.at[n], tp=to)

    w_near.wait_recv()

    @pl.when(core == 1)
    def _():
        ex_pair.start()

    @pl.when(core == 0)
    def _():
        ex_pair.wait_recv()
        for n, cut in enumerate(strips):
            cols = slice(width - apart + cut.start, width - apart + cut.stop)
            both = jnp.dot(att[1].reshape(half, -1), wg[t, :, cols], preferred_element_type=f32)
            both = both + jnp.dot(ae[...].reshape(half, -1), wg[t1, :, cols], preferred_element_type=f32)
            both = both.astype(bf16).reshape(GROUPS, 2, span, -1)
            for side in range(2):
                s_far[side, :, cut] = both[:, side].reshape(rows, -1)
                sums(n, side).start()

    over(lambda ids: absorb((0, [(spx - 2 * i, *late) for i in ids])))
    settle(0)
    for k in range(2):
        pass_on(k)
    ex_near = remote(att.at[0, :, 1 - core], ag.at[t], sent.at[5], a_r.at[0], tp=t1)
    ex_near.start()
    w_far.wait_recv()
    w_fwd = remote(wg.at[t2, :, alone], wg.at[t2, :, alone], sent.at[4], w_r.at[2], tp=t1)
    w_fwd.start()
    part[...] = jnp.dot(flat(att[0, :, core]), wg[t], preferred_element_type=f32)
    for k in range(2, SHARED):
        pass_on(k)
    ex_near.wait_recv()
    part[...] += jnp.dot(flat(ag[t1]), wg[t1], preferred_element_type=f32)
    ex_far.wait_recv()
    total = part[:, gathered] + jnp.dot(flat(ag[t2]), wg[t2, :, gathered], preferred_element_type=f32)
    ex_skew.wait_recv()
    w_fwd.wait_recv()
    drain(wg.at[0, :, : 2 * SHARED * unit], d_r)
    total = total + jnp.dot(flat(ag[t3]), wg[t3, :, gathered], preferred_element_type=f32)
    out[:, gathered] = total.astype(bf16)
    drain(wg.at[0:3, 0:rows], sent.at[0])

    @pl.when(c == 0)
    def _():
        drain(kv.at[0 : last_row + 1], sent.at[1])

    @pl.when(c == 1)
    def _():
        drain(kv.at[0:last_row], sent.at[1])

    drain(wg.at[0, :, : 4 * SHARED * unit], sent.at[2])
    w_near.wait_send()
    drain(wg.at[0, :, : 2 * alone.size], sent.at[4])
    drain(ag.at[0:3], sent.at[5])

    for n, cut in enumerate(strips):
        cols = slice(width - apart + cut.start, width - apart + cut.stop)
        sums(n, 0).wait_recv()
        out[:, cols] = (part[:, cols] + r_far[:, cut].astype(f32)).astype(bf16)

    @pl.when(core == 1)
    def _():
        ex_pair.wait_send()

    @pl.when(core == 0)
    def _():
        drain(s_far, sent.at[6])


def per_device(sp_size, tokens, w_query, w_key, w_value, w_out, cum_gate):
    rows, width = tokens.shape
    half, block = 2 * rows, 4 * rows
    heads = w_query.shape[1] // HD
    out_width = w_out.shape[1]
    extra = -(-(3 * heads + 3) // 16) * 16
    bf16, f32 = jnp.bfloat16, jnp.float32
    dma = pltpu.SemaphoreType.DMA
    anywhere = pl.BlockSpec(memory_space=pltpu.HBM)
    summed = (rows, out_width * 6 // 16)
    return pl.pallas_call(
        functools.partial(kernel, sp_size),
        out_shape=pltpu.VMEM((rows, out_width), bf16),
        in_specs=[anywhere] * 6,
        out_specs=pl.BlockSpec(memory_space=pltpu.VMEM),
        scratch_shapes=[
            pltpu.VMEM((2, GROUPS, 2, rows // GROUPS, width), bf16),
            pltpu.VMEM(w_query.shape, bf16),
            pltpu.VMEM((2 * HD, width), bf16),
            pltpu.VMEM((width, 2 * HD), bf16),
            pltpu.VMEM(cum_gate.shape, f32),
            pltpu.VMEM((sp_size, 2 * extra + block, 2 * HD), bf16),
            pltpu.VMEM((sp_size, block, 2 * HD), bf16),
            pltpu.VMEM((2, 4 * HD, heads * half), bf16),
            pltpu.VMEM((2, 8, heads * half), f32),
            pltpu.VMEM((2, HD + 16, heads * half), f32),
            pltpu.VMEM((2, GROUPS, 2, rows // GROUPS, heads * HD), bf16),
            pltpu.VMEM((rows, out_width), f32),
            pltpu.VMEM((2,) + summed, bf16), pltpu.VMEM(summed, bf16),
            pltpu.VMEM((4,) + w_out.shape, bf16),
            pltpu.VMEM((4, GROUPS, rows // GROUPS, w_out.shape[0]), bf16),
            pltpu.VMEM((GROUPS, 2, rows // GROUPS, w_out.shape[0]), bf16),
            dma((5,)), dma((7,)), dma((1,)), dma((CHUNKS,)), dma((GROUPS,)),
            dma((sp_size, 1 + GROUPS)), dma((2,)), pltpu.SemaphoreType.REGULAR,
            dma((3,)), dma((4,)), dma((SHARED,)), dma((SHARED,)), dma(()),
        ],
        compiler_params=pltpu.CompilerParams(
            collective_id=0, has_side_effects=True, vmem_limit_bytes=62 * 1024 * 1024
        ),
    )(tokens, w_query, w_key.T, w_value.T, w_out, cum_gate)


def solution(mesh):
    placed = (
        P(("sp", "tp"), None),
        P(None, "tp"),
        P(None, "tp"),
        P(None, "tp"),
        P("tp", None),
        P("tp", "sp"),
    )
    return jax.shard_map(
        functools.partial(per_device, mesh.shape["sp"]),
        mesh=mesh, in_specs=placed, out_specs=P(("sp", "tp"), None), check_vma=False,
    )
```

```python
import functools

import jax
import jax.numpy as jnp
from jax import lax
from jax.experimental import pallas as pl
from jax.experimental.pallas import tpu as pltpu
from jax.sharding import PartitionSpec as P

HD = 64
MESH = pl.DeviceIdType.MESH
CHUNKS = 4
GROUPS = 2
SHARED = 4
FAR = -1e30


def kernel(
    sp_size, tok, wq, wk, wv, wo, gate, out,
    x, wqv, wboth, wt, gv, kv, gk, qt, top, acc, att, part,
    s_far, r_far, wg, ag, ae,
    load, sent, tok_r, far_r, fwd_r, kv_r, o_r, ready, w_r, a_r, y_r, b_r, d_r,
):
    f32, bf16 = jnp.float32, jnp.bfloat16
    rows = tok.shape[0]
    half = 2 * rows
    block = 2 * half
    heads = wq.shape[1] // HD
    width = wo.shape[1]
    apart = r_far.shape[1]
    gathered = pl.ds(0, width - apart)
    unit = width // 16
    alone = pl.ds(2 * SHARED * unit, width - apart - 2 * SHARED * unit)
    sp = lax.axis_index("sp")
    t = lax.axis_index("tp")
    core = lax.rem(t, 2)
    p = t // 2
    t1 = t + 1 - 2 * core
    t2 = lax.rem(t + 2, 4)
    t3 = 3 - t
    r = sp // 2
    c = lax.rem(sp, 2)
    last_row = sp_size // 2 - 1
    spx = sp + 1 - 2 * c
    has_next = r < last_row

    def at(n, unit):
        return pl.ds(pl.multiple_of(n * unit, unit), unit)

    span = rows // GROUPS
    loads = [
        pltpu.make_async_copy(gate, gv, load.at[0]),
        pltpu.make_async_copy(wk, wboth.at[0:HD], load.at[1]),
        pltpu.make_async_copy(wv, wboth.at[HD : 2 * HD], load.at[1]),
        pltpu.make_async_copy(wq, wqv, load.at[2]),
        pltpu.make_async_copy(wo, wg.at[t], load.at[3]),
    ]
    arrive = [
        pltpu.make_async_copy(tok.at[pl.ds(n * span, span)], x.at[0, n, core], load.at[4])
        for n in range(GROUPS)
    ]
    for copy in arrive:
        copy.start()
    for copy in loads:
        copy.start()

    def drain(ref, semaphore):
        pltpu.make_async_copy(ref, ref, semaphore).wait()

    barrier = pltpu.get_barrier_semaphore()
    pl.semaphore_signal(barrier, inc=1, device_id={"tp": t1}, device_id_type=MESH)
    pl.semaphore_signal(barrier, inc=1, device_id={"tp": t2}, device_id_type=MESH)
    pl.semaphore_signal(barrier, inc=1, device_id={"tp": t3}, device_id_type=MESH)
    pl.semaphore_signal(barrier, inc=1, device_id={"sp": spx}, device_id_type=MESH)

    @pl.when(has_next)
    def _():
        pl.semaphore_signal(barrier, inc=1, device_id={"sp": sp + 2}, device_id_type=MESH)

    @pl.when(r > 0)
    def _():
        pl.semaphore_signal(barrier, inc=1, device_id={"sp": sp - 2}, device_id_type=MESH)

    drain(x.at[0, :, core], load.at[4])
    drain(wboth, load.at[1])
    wt[...] = wboth[...].T
    peers = 4 + jnp.where(has_next, 1, 0) + jnp.where(r > 0, 1, 0)
    pl.semaphore_wait(barrier, peers)

    step = rows // CHUNKS

    def piece(kind, n):
        return x.at[kind, n * step // span, core, pl.ds(n * step % span, step)]

    def remote(src, dst, ss, rs, **where):
        return pltpu.make_async_remote_copy(
            src_ref=src, dst_ref=dst, send_sem=ss, recv_sem=rs,
            device_id=where, device_id_type=MESH,
        )

    far = [
        remote(piece(0, n), piece(1, n), sent.at[0], far_r.at[n], tp=t2) for n in range(CHUNKS)
    ]
    for cp in far[: CHUNKS // GROUPS]:
        cp.start()
    mine = x.at[0, :, core]
    near = remote(mine, mine, sent.at[0], tok_r.at[0], tp=t1)
    near.start()

    def place(n):
        return lax.rem(n // span, 2) * rows + n // (2 * span) * span + lax.rem(n, span)

    loads[0].wait()
    g = gv[...]
    lanes = [slice(core_n * rows + n * span, core_n * rows + (n + 1) * span) for n in range(GROUPS) for core_n in range(2)]
    sides = (jnp.where(p == 0, g[:, :half], g[:, half:]), jnp.where(p == 0, g[:, half:], g[:, :half]))
    extra = (kv.shape[1] - block) // 2
    zeros = jnp.zeros(gk.shape[2:], bf16)
    index = lax.broadcasted_iota(jnp.int32, (extra, half), 0)
    for kind, gs in enumerate(sides):
        gs = jnp.concatenate([gs[:, cut] for cut in lanes], axis=1)
        hi = gs.astype(bf16).astype(f32)
        mid = (gs - hi).astype(bf16).astype(f32)
        low = (gs - hi - mid).astype(bf16).astype(f32)
        parts = (hi, mid, low)
        key_side = jnp.where((index >= 3 * heads) & (index < 3 * heads + 3), 1.0, 0.0).astype(f32)
        for k in range(3):
            for h in range(heads):
                key_side = jnp.where(index == k * heads + h, -parts[k][h : h + 1, :], key_side)
        kv[sp, kind * extra : (kind + 1) * extra, :] = key_side.astype(bf16)
        qt[kind] = jnp.zeros(qt.shape[1:], bf16)
        for h in range(heads):
            side = jnp.where((index < 3 * heads) & (lax.rem(index, heads) == h), 1.0, 0.0).astype(f32)
            for k in range(3):
                side = jnp.where(index == 3 * heads + k, parts[k][h : h + 1, :], side)
            qt[kind, 2 * HD : 2 * HD + extra, h * half : (h + 1) * half] = side.astype(bf16)

    def unpack(src):
        for kind in range(2):
            lines = kv[src, kind * extra : (kind + 1) * extra, :]
            wide = jnp.concatenate([lines, jnp.zeros((gk.shape[2] - extra, half), bf16)], axis=0)
            gk[src, kind * half : (kind + 1) * half, :] = wide.T

    bounds = (0, half, half + half // GROUPS, block)
    lead = 2 * extra

    def project_kv(part_n):
        lo, hi_row = bounds[part_n], bounds[part_n + 1]
        xs = x[0] if part_n == 0 else x[1, part_n - 1]
        both = jnp.dot(xs.reshape(hi_row - lo, x.shape[-1]), wt[...], preferred_element_type=f32)
        kv[sp, lead + lo : lead + hi_row, :] = both.astype(bf16)

    def project_q(kind):
        xs = x[kind].reshape(half, x.shape[-1])
        q = jnp.dot(xs, wqv[...], preferred_element_type=f32).astype(bf16).astype(f32)
        q = (q * (float(HD) ** -0.5)).T.astype(bf16)
        for h in range(heads):
            qt[kind, 0:HD, h * half : (h + 1) * half] = q[h * HD : (h + 1) * HD]

    def message(src, n):
        return kv.at[src, 0 if n == 0 else lead + bounds[n] : lead + bounds[n + 1]]

    def along(src, n, row):
        ref = message(src, n)
        return remote(ref, ref, sent.at[1], kv_r.at[src, n], sp=2 * row + c)

    def across(src, n):
        ref = message(src, n)
        return remote(ref, ref, sent.at[1], kv_r.at[src, n], sp=spx)

    def send_own(n):
        @pl.loop(0, last_row - r)
        def _(i):
            along(sp, n, last_row - i).start()

        @pl.when(c == 0)
        def _():
            across(sp, n).start()

    def hear():
        @pl.when(r < last_row - 1)
        def _():
            pl.semaphore_wait(ready, 1)

    @pl.when(r > 0)
    def _():
        hear()

        @pl.when(has_next)
        def _():
            pl.semaphore_signal(ready, inc=1, device_id={"sp": sp - 2}, device_id_type=MESH)

    def positions(shape, axis, kind, offset):
        n = lax.rem(lax.broadcasted_iota(jnp.int32, shape, axis), half) + offset
        return place(n) + (p if kind == 0 else 1 - p) * half

    def absorb(*groups, first=()):
        held = {}
        scores = []
        for kind, pieces in groups:
            name = tuple((id(src), lo, hi_row) for src, lo, hi_row in pieces)
            if name not in held:
                keys = jnp.concatenate([kv[src, lead + lo : lead + hi_row, :] for src, lo, hi_row in pieces], axis=0)
                tails = jnp.concatenate([gk[src, lo:hi_row, :] for src, lo, hi_row in pieces], axis=0)
                ones = jnp.ones((16, keys.shape[0]), bf16)
                held[name] = (
                    jnp.concatenate([keys, tails], axis=1),
                    jnp.concatenate([keys.T[HD:], ones], axis=0),
                )
            s = jnp.dot(held[name][0], qt[kind], preferred_element_type=f32)
            cuts, n = [], 0
            for src, lo, hi_row in pieces:
                cut = s[n : n + hi_row - lo]
                n += hi_row - lo
                if src is sp:
                    key_kind = 0 if lo < half else 1
                    key_pos = positions((cut.shape[0], 1), 0, key_kind, lo % half)
                    query_pos = positions((1, cut.shape[1]), 1, kind, 0)
                    cut = jnp.where(key_pos <= query_pos, cut, FAR)
                cuts.append(cut)
            scores.append((name, cuts))
        tops = []
        for (kind, _), (_, cuts) in zip(groups, scores):
            peak = None if kind in first else top[kind, 0:1, :]
            for s in cuts:
                high = jnp.max(s, axis=0, keepdims=True)
                peak = high if peak is None else jnp.maximum(peak, high)
            tops.append(peak)
        weights = [
            jnp.concatenate([jnp.exp(s - peak).astype(bf16) for s in cuts], axis=0)
            for peak, (_, cuts) in zip(tops, scores)
        ]
        for peak, w, (kind, _), (name, _) in zip(tops, weights, groups, scores):
            total = jnp.dot(held[name][1], w, preferred_element_type=f32)
            if kind not in first:
                total = total + acc[kind] * jnp.exp(top[kind, 0:1, :] - peak)
            acc[kind] = total
            top[kind, 0:1, :] = peak

    def over(work):
        @pl.loop(0, r // 3)
        def _(j):
            work([3 * j + 1, 3 * j + 2, 3 * j + 3])

        @pl.when(r % 3 == 1)
        def _():
            work([r])

        @pl.when(r % 3 == 2)
        def _():
            work([r - 1, r])

    def strip(k, side):
        return pl.ds(pl.multiple_of((side * SHARED + k) * unit, unit), unit)

    def over_x(k, side):
        ref = wg.at[t2, :, strip(k, side)]
        return remote(ref, ref, sent.at[2], b_r.at[k], sp=spx)

    def over_chip(k, side, n):
        ref = wg.at[t2, :, strip(k, side)]
        return remote(ref, ref, sent.at[2], d_r, tp=t1)

    def share(k):
        c_far[k].wait_recv()
        over_x(k, c).start()
        over_chip(k, c, 0).start()

    def pass_on(k):
        over_x(k, 1 - c).wait_recv()
        over_chip(k, 1 - c, 1).start()

    def forward(n):
        far[n].wait_recv()
        cp = remote(piece(1, n), piece(1, n), sent.at[0], fwd_r.at[n * step // span], tp=t1)
        cp.start()
        return cp

    def relay(n):
        @pl.loop(1, r + 1)
        def _(i):
            across(sp - 2 * i, n).wait_recv()
            across(sp - 2 * i, n).start()

    first_part, early, late, other = [(0, half), (half, bounds[2]), (bounds[2], block), (half, block)]

    near.wait_recv()

    @pl.when(core == 0)
    def _():
        for cp in far[CHUNKS // GROUPS :]:
            cp.start()

    project_kv(0)

    @pl.when(r == 0)
    def _():
        hear()

    send_own(0)
    loads[3].wait()
    project_q(0)

    @pl.when(core == 1)
    def _():
        for cp in far[CHUNKS // GROUPS :]:
            cp.start()

    unpack(sp)
    absorb((0, [(sp, *first_part)]), first=(0,))
    fwd = [forward(0), forward(1)]

    @pl.when(c == 1)
    def _():
        across(spx, 0).wait_recv()
        unpack(spx)
        absorb((0, [(spx, *first_part)]))

    relay(0)
    loads[4].wait()
    c_far, w_far = [], remote(wg.at[t, :, alone], wg.at[t, :, alone], sent.at[4], w_r.at[1], tp=t2)
    for k in range(SHARED):
        ref = wg.at[t, :, strip(k, c)]
        c_far.append(remote(ref, ref, sent.at[2], y_r.at[k], tp=t2))
        c_far[k].start()
    drain(x.at[1, 0, 1 - core], fwd_r.at[0])
    project_kv(1)
    send_own(1)
    fwd.append(forward(2))

    def directs(ids):
        srcs = [sp - 2 * i for i in ids]
        for src in srcs:
            unpack(src)
        absorb((0, [(src, *first_part) for src in srcs]))

    over(directs)
    fwd.append(forward(3))
    absorb((0, [(sp, *early)]))
    drain(x.at[1, 1, 1 - core], fwd_r.at[1])
    project_kv(2)
    send_own(2)
    project_q(1)
    relay(1)

    @pl.when(core == 1)
    def _():
        share(0)

    @pl.when(c == 0)
    def _():
        absorb((1, [(sp, *first_part), (sp, *other)]), (0, [(sp, *late)]), first=(1,))

    @pl.when(c == 1)
    def _():
        across(spx, 1).wait_recv()
        absorb(
            (1, [(sp, *first_part), (sp, *other), (spx, 0, bounds[2])]),
            (0, [(sp, *late), (spx, *early)]), first=(1,),
        )

    def closer(ids):
        near_by = [sp - 2 * i for i in ids]
        absorb(
            (1, [(src, 0, bounds[2]) for src in near_by]),
            (0, [(src, *early) for src in near_by]),
        )

    over(closer)
    relay(2)
    w_near = remote(wg.at[t], wg.at[t], sent.at[3], w_r.at[0], tp=t1)
    w_near.start()

    @pl.when(core == 0)
    def _():
        share(0)

    share(1)

    def beyond_x(ids):
        beyond = [spx - 2 * i for i in ids]
        for src in beyond:
            across(src, 0).wait_recv()
            unpack(src)
        pieces = [(src, *first_part) for src in beyond]
        absorb((1, pieces), (0, pieces))

    over(beyond_x)

    @pl.when(c == 1)
    def _():
        across(spx, 2).wait_recv()
        absorb((1, [(spx, *late)]), (0, [(spx, *late)]))

    w_far.start()

    def nearly(ids):
        near_by, beyond = [sp - 2 * i for i in ids], [spx - 2 * i for i in ids]
        for src in beyond:
            across(src, 1).wait_recv()
        pieces = [(src, *late) for src in near_by] + [(src, *early) for src in beyond]
        absorb((1, pieces), (0, pieces))

    over(nearly)
    for k in range(2, SHARED):
        share(k)

    def lasts(ids):
        beyond = [spx - 2 * i for i in ids]
        for src in beyond:
            across(src, 2).wait_recv()
        absorb((1, [(src, *late) for src in beyond]))

    over(lasts)

    def settle(kind):
        rest = acc[kind, 0:HD, :] / acc[kind, HD : HD + 1, :]
        heads_up = jnp.concatenate([rest[:, h * half : (h + 1) * half] for h in range(heads)], axis=0)
        att[kind] = heads_up.T.astype(bf16).reshape(att.shape[1:])

    settle(1)
    theirs, others = att.at[1, :, core], att.at[1, :, 1 - core]
    ex_far = remote(theirs, ag.at[t], sent.at[5], a_r.at[1], tp=t2)
    ex_far.start()
    ex_skew = remote(others, ag.at[t], sent.at[5], a_r.at[2], tp=t3)
    ex_skew.start()

    def flat(value):
        return value.reshape(rows, value.shape[-1])

    middle = apart // 256 * 128
    strips = (slice(0, middle), slice(middle, apart))
    ex_pair = remote(att.at[1], ae, sent.at[6], a_r.at[3], tp=t1)

    def sums(n, side):
        to = t2 if side == 0 else t3
        cut = strips[n]
        return remote(s_far.at[side, :, cut], r_far.at[:, cut], sent.at[6], o_r.at[n], tp=to)

    w_near.wait_recv()

    @pl.when(core == 1)
    def _():
        ex_pair.start()

    @pl.when(core == 0)
    def _():
        ex_pair.wait_recv()
        for n, cut in enumerate(strips):
            cols = slice(width - apart + cut.start, width - apart + cut.stop)
            both = jnp.dot(att[1].reshape(half, -1), wg[t, :, cols], preferred_element_type=f32)
            both = both + jnp.dot(ae[...].reshape(half, -1), wg[t1, :, cols], preferred_element_type=f32)
            both = both.astype(bf16).reshape(GROUPS, 2, span, -1)
            for side in range(2):
                s_far[side, :, cut] = both[:, side].reshape(rows, -1)
                sums(n, side).start()

    over(lambda ids: absorb((0, [(spx - 2 * i, *late) for i in ids])))
    settle(0)
    for k in range(2):
        pass_on(k)
    ex_near = remote(att.at[0, :, 1 - core], ag.at[t], sent.at[5], a_r.at[0], tp=t1)
    ex_near.start()
    w_far.wait_recv()
    w_fwd = remote(wg.at[t2, :, alone], wg.at[t2, :, alone], sent.at[4], w_r.at[2], tp=t1)
    w_fwd.start()
    part[...] = jnp.dot(flat(att[0, :, core]), wg[t], preferred_element_type=f32)
    for k in range(2, SHARED):
        pass_on(k)
    ex_near.wait_recv()
    part[...] += jnp.dot(flat(ag[t1]), wg[t1], preferred_element_type=f32)
    ex_far.wait_recv()
    total = part[:, gathered] + jnp.dot(flat(ag[t2]), wg[t2, :, gathered], preferred_element_type=f32)
    ex_skew.wait_recv()
    w_fwd.wait_recv()
    drain(wg.at[0, :, : 2 * SHARED * unit], d_r)
    total = total + jnp.dot(flat(ag[t3]), wg[t3, :, gathered], preferred_element_type=f32)
    out[:, gathered] = total.astype(bf16)
    drain(wg.at[0:3, 0:rows], sent.at[0])

    @pl.when(c == 0)
    def _():
        drain(kv.at[0 : last_row + 1], sent.at[1])

    @pl.when(c == 1)
    def _():
        drain(kv.at[0:last_row], sent.at[1])

    drain(wg.at[0, :, : 4 * SHARED * unit], sent.at[2])
    w_near.wait_send()
    drain(wg.at[0, :, : 2 * alone.size], sent.at[4])
    drain(ag.at[0:3], sent.at[5])

    for n, cut in enumerate(strips):
        cols = slice(width - apart + cut.start, width - apart + cut.stop)
        sums(n, 0).wait_recv()
        out[:, cols] = (part[:, cols] + r_far[:, cut].astype(f32)).astype(bf16)

    @pl.when(core == 1)
    def _():
        ex_pair.wait_send()

    @pl.when(core == 0)
    def _():
        drain(s_far, sent.at[6])


def per_device(sp_size, tokens, w_query, w_key, w_value, w_out, cum_gate):
    rows, width = tokens.shape
    half, block = 2 * rows, 4 * rows
    heads = w_query.shape[1] // HD
    out_width = w_out.shape[1]
    extra = -(-(3 * heads + 3) // 16) * 16
    bf16, f32 = jnp.bfloat16, jnp.float32
    dma = pltpu.SemaphoreType.DMA
    anywhere = pl.BlockSpec(memory_space=pltpu.HBM)
    summed = (rows, out_width * 6 // 16)
    return pl.pallas_call(
        functools.partial(kernel, sp_size),
        out_shape=pltpu.VMEM((rows, out_width), bf16),
        in_specs=[anywhere] * 6,
        out_specs=pl.BlockSpec(memory_space=pltpu.VMEM),
        scratch_shapes=[
            pltpu.VMEM((2, GROUPS, 2, rows // GROUPS, width), bf16),
            pltpu.VMEM(w_query.shape, bf16),
            pltpu.VMEM((2 * HD, width), bf16),
            pltpu.VMEM((width, 2 * HD), bf16),
            pltpu.VMEM(cum_gate.shape, f32),
            pltpu.VMEM((sp_size, 2 * extra + block, 2 * HD), bf16),
            pltpu.VMEM((sp_size, block, 2 * HD), bf16),
            pltpu.VMEM((2, 4 * HD, heads * half), bf16),
            pltpu.VMEM((2, 8, heads * half), f32),
            pltpu.VMEM((2, HD + 16, heads * half), f32),
            pltpu.VMEM((2, GROUPS, 2, rows // GROUPS, heads * HD), bf16),
            pltpu.VMEM((rows, out_width), f32),
            pltpu.VMEM((2,) + summed, bf16), pltpu.VMEM(summed, bf16),
            pltpu.VMEM((4,) + w_out.shape, bf16),
            pltpu.VMEM((4, GROUPS, rows // GROUPS, w_out.shape[0]), bf16),
            pltpu.VMEM((GROUPS, 2, rows // GROUPS, w_out.shape[0]), bf16),
            dma((5,)), dma((7,)), dma((1,)), dma((CHUNKS,)), dma((GROUPS,)),
            dma((sp_size, 1 + GROUPS)), dma((2,)), pltpu.SemaphoreType.REGULAR,
            dma((3,)), dma((4,)), dma((SHARED,)), dma((SHARED,)), dma(()),
        ],
        compiler_params=pltpu.CompilerParams(
            collective_id=0, has_side_effects=True, vmem_limit_bytes=62 * 1024 * 1024
        ),
    )(tokens, w_query, w_key.T, w_value.T, w_out, cum_gate)


def solution(mesh):
    placed = (
        P(("sp", "tp"), None),
        P(None, "tp"),
        P(None, "tp"),
        P(None, "tp"),
        P("tp", None),
        P("tp", "sp"),
    )
    return jax.shard_map(
        functools.partial(per_device, mesh.shape["sp"]),
        mesh=mesh, in_specs=placed, out_specs=P(("sp", "tp"), None), check_vma=False,
    )
```
